32 devices in a mesh: rep: 2 (over x), fs: 8 (over z, y), tp: 2 (over core).
Axes of the slice: x: 2, y: 2, z: 4, core: 2. Of those that a mesh axis runs over, the one named last changes fastest.
Arguments:
- pre_gate: bfloat16 [12288, 4096], P(('rep', 'fs'), 'tp'), may hold values from -6 to 6
- pre_linear: bfloat16 [12288, 4096], P(('rep', 'fs'), 'tp'), may hold values from -6 to 6
- taps_gate: float32 [3, 4096], P(None, 'tp'), may hold values from -3.5 to 3.5
- taps_linear: float32 [3, 4096], P(None, 'tp'), may hold values from -3.5 to 3.5
- bias_gate: float32 [4096], P('tp'), may hold values from -3 to 3
- bias_linear: float32 [4096], P('tp'), may hold values from -3 to 3
- down_weight: bfloat16 [4096, 2048], P('tp', 'fs'), may hold values from -0.09375 to 0.09375
- out_grad: bfloat16 [12288, 2048], P(('rep', 'fs')), may hold values from -8 to 8
Outputs:
- grad_gate: bfloat16 [12288, 4096], P(('rep', 'fs'), 'tp')
- grad_linear: bfloat16 [12288, 4096], P(('rep', 'fs'), 'tp')
- grad_taps_gate: float32 [3, 4096], P(None, 'tp')
- grad_taps_linear: float32 [3, 4096], P(None, 'tp')
- grad_bias_gate: float32 [4096], P('tp')
- grad_bias_linear: float32 [4096], P('tp')
- grad_down: float32 [4096, 2048], P('tp', 'fs')
- row_norms: float32 [4096], P('tp')
The draws below stay inside these ranges and needn't reach their ends.
All inputs are finite; a program needn't handle non-finite values.
Results may differ from the reference program's by a relative error of at most 0.0031.
Values may be sent and summed in bfloat16 or wider, within the bound.
A program may use at most 128 MiB of HBM per device.

```python
import jax
import jax.numpy as jnp

D = 2048
FF = 4096
KERNEL = 3
TOK_DEV = 768
TOKENS = 12288


def raised(entries, key, source, target, blocks, factor):
    owner, partner = [(jnp.arange(entries.shape[axis_at]) // (entries.shape[axis_at] // blocks)).reshape([-1 if axis == axis_at else 1 for axis in range(entries.ndim)]) for axis_at in (source, target)]
    chosen = jax.random.permutation(key, blocks)[partner]
    strong = (owner == chosen) | (owner == (partner + blocks // 2) % blocks)
    return jnp.where(strong, factor * entries, entries)


def levels(rng, dims, cuts, low, high):
    gain, own = 1.0, jax.random.fold_in(rng, 6)
    for position, blocks in cuts:
        draws = jnp.exp(jax.random.uniform(jax.random.fold_in(own, position), (blocks,), jnp.float32, low / len(cuts), high / len(cuts)))
        gain = gain * jnp.repeat(draws, dims[position] // blocks).reshape([-1 if axis == position else 1 for axis in range(len(dims))])
    return gain


def bell_draw(own_key, shape, scale, limit, shards=(), kind=jnp.bfloat16):
    entries = scale * jax.random.normal(own_key, shape, jnp.float32)
    if shards:
        entries = entries * levels(own_key, shape, shards, -0.22, 0.18)
    return jnp.clip(entries, -limit, limit).astype(kind)


def heavy_noise(key, dims, deviation, most, pieces, heavy, kind=jnp.bfloat16):
    entries = deviation * jax.random.normal(key, dims, jnp.float32)
    if pieces:
        entries = entries * levels(key, dims, pieces, -0.22, 0.18)
    return jnp.clip(raised(entries, jax.random.fold_in(key, 3), *heavy), -most, most).astype(kind)


def setup_inputs(seed: int = 0) -> dict:
    seeds = jax.random.split(jax.random.key(seed), 9)
    return {
        "pre_gate": bell_draw(seeds[0], (TOKENS, FF), 1.0, 6.0, ((0, 16), (1, 2))),
        "pre_linear": bell_draw(seeds[1], (TOKENS, FF), 1.0, 6.0, ((0, 16), (1, 2))),
        "taps_gate": bell_draw(seeds[2], (KERNEL, FF), KERNEL ** -0.5, 3.5, ((1, 2),), jnp.float32),
        "taps_linear": bell_draw(seeds[3], (KERNEL, FF), KERNEL ** -0.5, 3.5, ((1, 2),), jnp.float32),
        "bias_gate": bell_draw(seeds[4], (FF,), 0.5, 3.0, ((0, 2),), jnp.float32),
        "bias_linear": bell_draw(seeds[5], (FF,), 0.5, 3.0, ((0, 2),), jnp.float32),
        "down_weight": bell_draw(seeds[6], (FF, D), FF ** -0.5, 0.09375, ((0, 2), (1, 8))),
        "out_grad": heavy_noise(seeds[7], (TOKENS, D), 1.0, 8.0, ((0, 16),), (0, 1, 16, 2.0)),
    }


def convolve(values, taps, bias):
    length = values.shape[1]
    padded = jnp.pad(values, ((0, 0), (2, 0), (0, 0)))
    return taps[0] * padded[:, 0:length] + taps[1] * padded[:, 1:length + 1] + taps[2] * padded[:, 2:length + 2] + bias


def convolve_back(grads, taps):
    length = grads.shape[1]
    padded = jnp.pad(grads, ((0, 0), (0, 2), (0, 0)))
    return taps[0] * padded[:, 2:length + 2] + taps[1] * padded[:, 1:length + 1] + taps[2] * padded[:, 0:length]


def tap_grads(grads, values):
    length = values.shape[1]
    padded = jnp.pad(values, ((0, 0), (2, 0), (0, 0)))
    return jnp.stack([jnp.sum(grads * padded[:, j:j + length], axis=(0, 1)) for j in range(3)])


def reference(pre_gate, pre_linear, taps_gate, taps_linear, bias_gate, bias_linear, down_weight, out_grad):
    seqs = pre_gate.shape[0] // TOK_DEV
    width = pre_gate.shape[1]
    gate_in = pre_gate.astype(jnp.float32).reshape(seqs, TOK_DEV, width)
    linear_in = pre_linear.astype(jnp.float32).reshape(seqs, TOK_DEV, width)
    gate_pre = convolve(gate_in, taps_gate, bias_gate)
    linear_pre = convolve(linear_in, taps_linear, bias_linear)
    sigma = jax.nn.sigmoid(gate_pre)
    silu_val = gate_pre * sigma
    hidden = (silu_val * linear_pre).astype(jnp.bfloat16).reshape(seqs * TOK_DEV, width)
    grad_hidden = jnp.dot(out_grad, down_weight.T, preferred_element_type=jnp.float32).reshape(seqs, TOK_DEV, width)
    grad_gate_pre = grad_hidden * linear_pre * sigma * (1.0 + gate_pre * (1.0 - sigma))
    grad_linear_pre = grad_hidden * silu_val
    grad_gate = convolve_back(grad_gate_pre, taps_gate).reshape(seqs * TOK_DEV, width).astype(jnp.bfloat16)
    grad_linear = convolve_back(grad_linear_pre, taps_linear).reshape(seqs * TOK_DEV, width).astype(jnp.bfloat16)
    grad_taps_gate = tap_grads(grad_gate_pre, gate_in)
    grad_taps_linear = tap_grads(grad_linear_pre, linear_in)
    grad_bias_gate = jnp.sum(grad_gate_pre, axis=(0, 1))
    grad_bias_linear = jnp.sum(grad_linear_pre, axis=(0, 1))
    grad_down = jnp.dot(hidden.T, out_grad, preferred_element_type=jnp.float32)
    row_norms = jnp.sum(grad_down * grad_down, axis=1)
    return (grad_gate, grad_linear, grad_taps_gate, grad_taps_linear, grad_bias_gate, grad_bias_linear, grad_down, row_norms)
```

```python
import functools

import jax
import jax.numpy as jnp
from jax import lax
from jax.experimental import pallas as pl
from jax.experimental.pallas import tpu as pltpu
from jax.sharding import PartitionSpec as P

MESH = pl.DeviceIdType.MESH


def shift_down(values, steps):
    if steps == 0:
        return values
    rows = lax.broadcasted_iota(jnp.int32, values.shape, 0)
    return jnp.where(rows < steps, 0.0, pltpu.roll(values, steps, 0))


def shift_up(values, steps):
    length = values.shape[0]
    rows = lax.broadcasted_iota(jnp.int32, values.shape, 0)
    return jnp.where(rows >= length - steps, 0.0, pltpu.roll(values, length - steps, 0))


def conv_chunk(values, taps, bias):
    return (
        taps[0:1] * shift_down(values, 2)
        + taps[1:2] * shift_down(values, 1)
        + taps[2:3] * values
        + bias
    )


def conv_back_chunk(grads, taps):
    return taps[0:1] * shift_up(grads, 2) + taps[1:2] * shift_up(grads, 1) + taps[2:3] * grads


def kernel(
    fs, chunk,
    pg_ref, pl_ref, tg_ref, tl_ref, bg_ref, bl_ref, w_ref, og_ref,
    gg_ref, gl_ref, cp_ref, gd_ref, rn_ref,
    wbuf, sbuf, pbuf, rbuf, xs, xr, cpbuf, cps, cpx, rnbuf,
    w_send, w_recv, y_send, y_recv, p_send, p_recv, f_send, f_recv, s_send, s_recv, x_send, x_recv,
    c_send, c_recv, cx_send, cx_recv, n_send, n_recv,
):
    me = lax.axis_index("fs")
    rep = lax.axis_index("rep")
    partner = 1 - rep
    pairs = fs // 2
    z = me // 2
    par = me % 2
    mate = me + 1 - 2 * par
    tokens, ff = pg_ref.shape
    dc = w_ref.shape[1]
    chunks = ff // chunk
    half = ff // 2
    lag = chunks // 2
    per = -(-(fs - 1) // chunks)

    def to(k):
        return lax.rem(me + k, fs)

    def rows_of(c):
        return pl.ds(pl.multiple_of(c * chunk, chunk), chunk)

    def shard(z_at, parity):
        return z_at * 2 + parity

    def z_to(k):
        return lax.rem(z + k, pairs)

    def z_from(k):
        return lax.rem(z + pairs - k, pairs)

    def my_half():
        return pl.ds(pl.multiple_of(rep * half, half), half)

    def w_copy(k):
        return pltpu.make_async_remote_copy(
            src_ref=w_ref.at[my_half()], dst_ref=wbuf.at[me, my_half()],
            send_sem=w_send.at[k], recv_sem=w_recv.at[k],
            device_id={"fs": shard(z_to(k), par)}, device_id_type=MESH)

    def y_first():
        return pltpu.make_async_remote_copy(
            src_ref=w_ref.at[my_half()], dst_ref=wbuf.at[me, my_half()],
            send_sem=y_send.at[0], recv_sem=y_recv.at[0],
            device_id={"fs": mate}, device_id_type=MESH)

    def y_copy(k):
        block = wbuf.at[shard(z_from(k), par), my_half()]
        return pltpu.make_async_remote_copy(
            src_ref=block, dst_ref=block,
            send_sem=y_send.at[k], recv_sem=y_recv.at[k],
            device_id={"fs": mate}, device_id_type=MESH)

    def f_copy(item):
        block = wbuf.at[shard(z_from(item % pairs), (par + item // pairs) % 2), my_half()]
        return pltpu.make_async_remote_copy(
            src_ref=block, dst_ref=block,
            send_sem=f_send.at[item], recv_sem=f_recv.at[item],
            device_id={"rep": partner}, device_id_type=MESH)

    def p_copy(c):
        return pltpu.make_async_remote_copy(
            src_ref=sbuf.at[1 - par, :, rows_of(c)], dst_ref=pbuf.at[:, rows_of(c)],
            send_sem=p_send.at[c], recv_sem=p_recv.at[c],
            device_id={"fs": mate}, device_id_type=MESH)

    def s_copy(c, k):
        return pltpu.make_async_remote_copy(
            src_ref=sbuf.at[par, z_to(k), rows_of(c)], dst_ref=rbuf.at[k, rows_of(c)],
            send_sem=s_send.at[c, k], recv_sem=s_recv.at[c, k],
            device_id={"fs": shard(z_to(k), par)}, device_id_type=MESH)

    def pair_sum(c):
        p_copy(c).wait_recv()
        for at in range(pairs):
            both = sbuf[par, at, rows_of(c)].astype(jnp.float32) + pbuf[at, rows_of(c)].astype(jnp.float32)
            sbuf[par, at, rows_of(c)] = both.astype(jnp.bfloat16)

        @pl.loop(1, pairs)
        def _(k):
            s_copy(c, k).start()

    def x_copy(c):
        return pltpu.make_async_remote_copy(
            src_ref=xs.at[rows_of(c)], dst_ref=xr.at[rows_of(c)],
            send_sem=x_send.at[c], recv_sem=x_recv.at[c],
            device_id={"rep": partner}, device_id_type=MESH)

    def c_copy(k):
        return pltpu.make_async_remote_copy(
            src_ref=cpbuf.at[me], dst_ref=cpbuf.at[me],
            send_sem=c_send.at[k], recv_sem=c_recv.at[k],
            device_id={"fs": to(k)}, device_id_type=MESH)

    def cx_copy():
        return pltpu.make_async_remote_copy(
            src_ref=cps, dst_ref=cpx, send_sem=cx_send, recv_sem=cx_recv,
            device_id={"rep": partner}, device_id_type=MESH)

    def n_copy(k):
        return pltpu.make_async_remote_copy(
            src_ref=rnbuf.at[me], dst_ref=rnbuf.at[me],
            send_sem=n_send.at[k], recv_sem=n_recv.at[k],
            device_id={"fs": to(k)}, device_id_type=MESH)

    barrier = pltpu.get_barrier_semaphore()

    @pl.loop(1, fs)
    def _(k):
        pl.semaphore_signal(barrier, inc=1, device_id={"fs": to(k)}, device_id_type=MESH)

    pl.semaphore_signal(barrier, inc=1, device_id={"rep": partner}, device_id_type=MESH)
    pl.semaphore_wait(barrier, fs)

    y_first().start()

    @pl.loop(1, pairs)
    def _(k):
        w_copy(k).start()

    wbuf[me] = w_ref[...]

    @pl.loop(0, chunks)
    def _(c):
        cols = rows_of(c)
        gate_pre = conv_chunk(
            pg_ref[:, cols].astype(jnp.float32), tg_ref[:, cols], bg_ref[:, cols])
        linear_pre = conv_chunk(
            pl_ref[:, cols].astype(jnp.float32), tl_ref[:, cols], bl_ref[:, cols])
        hidden = (gate_pre * jax.nn.sigmoid(gate_pre) * linear_pre).astype(jnp.bfloat16)
        for j in range(fs):
            part = lax.dot_general(
                hidden, og_ref[:, j * dc:(j + 1) * dc], (((0,), (0,)), ((), ())),
                preferred_element_type=jnp.float32)
            sbuf[j % 2, j // 2, cols] = part.astype(jnp.bfloat16)

        p_copy(c).start()

        @pl.when(c >= lag)
        def _():
            pair_sum(c - lag)

        for step in range(per):
            k = c * per + step + 1

            @pl.when(k < pairs)
            def _():
                w_copy(k).wait_recv()
                y_copy(k).start()
                f_copy(k).start()

            @pl.when((k >= pairs) & (k < fs))
            def _():
                y_copy(k - pairs).wait_recv()
                f_copy(k).start()

    @pl.loop(1, fs)
    def _(k):
        f_copy(k).wait_recv()

    @pl.loop(0, chunks)
    def _(c):
        cols = rows_of(c)
        gate_in = pg_ref[:, cols].astype(jnp.float32)
        linear_in = pl_ref[:, cols].astype(jnp.float32)
        taps_gate, taps_linear = tg_ref[:, cols], tl_ref[:, cols]
        gate_pre = conv_chunk(gate_in, taps_gate, bg_ref[:, cols])
        linear_pre = conv_chunk(linear_in, taps_linear, bl_ref[:, cols])
        sigma = jax.nn.sigmoid(gate_pre)
        grad_hidden = jnp.zeros((tokens, chunk), jnp.float32)
        for j in range(fs):
            grad_hidden += lax.dot_general(
                og_ref[:, j * dc:(j + 1) * dc], wbuf[j, cols], (((1,), (1,)), ((), ())),
                preferred_element_type=jnp.float32)
        grad_gate_pre = grad_hidden * linear_pre * sigma * (1.0 + gate_pre * (1.0 - sigma))
        grad_linear_pre = grad_hidden * (gate_pre * sigma)
        gg_ref[:, cols] = conv_back_chunk(grad_gate_pre, taps_gate).astype(jnp.bfloat16)
        gl_ref[:, cols] = conv_back_chunk(grad_linear_pre, taps_linear).astype(jnp.bfloat16)
        for j in range(3):
            cpbuf[me, j:j + 1, cols] = jnp.sum(
                grad_gate_pre * shift_down(gate_in, 2 - j), axis=0, keepdims=True)
            cpbuf[me, j + 3:j + 4, cols] = jnp.sum(
                grad_linear_pre * shift_down(linear_in, 2 - j), axis=0, keepdims=True)
        cpbuf[me, 6:7, cols] = jnp.sum(grad_gate_pre, axis=0, keepdims=True)
        cpbuf[me, 7:8, cols] = jnp.sum(grad_linear_pre, axis=0, keepdims=True)

        @pl.when(c == chunks - 1)
        def _():
            @pl.loop(1, fs)
            def _(k):
                c_copy(k).start()

        @pl.when(c < lag)
        def _():
            pair_sum(chunks - lag + c)

        total = sbuf[par, z, cols].astype(jnp.float32)
        for k in range(1, pairs):
            s_copy(c, k).wait_recv()
            total += rbuf[k, cols].astype(jnp.float32)
        xs[cols] = total
        x_copy(c).start()

    @pl.loop(1, fs)
    def _(k):
        c_copy(k).wait_recv()

    sums = cpbuf[0]
    for j in range(1, fs):
        sums += cpbuf[j]
    cps[...] = sums
    cx_copy().start()

    @pl.loop(0, chunks)
    def _(c):
        rows = rows_of(c)
        x_copy(c).wait_recv()
        total = xs[rows] + xr[rows]
        gd_ref[rows] = total
        square = total * total
        while square.shape[1] % 256 == 0:
            middle = square.shape[1] // 2
            square = square[:, :middle] + square[:, middle:]
        rnbuf[me, 0:1, rows] = jnp.sum(square.T, axis=0, keepdims=True)

    @pl.loop(1, fs)
    def _(k):
        n_copy(k).start()

    cx_copy().wait_recv()
    cp_ref[...] = cps[...] + cpx[...]

    @pl.loop(1, fs)
    def _(k):
        n_copy(k).wait_recv()

    norms = rnbuf[0]
    for j in range(1, fs):
        norms += rnbuf[j]
    rn_ref[...] = norms

    cx_copy().wait_send()
    y_first().wait_send()

    @pl.loop(1, pairs)
    def _(k):
        w_copy(k).wait_send()
        y_copy(k).wait_send()

    @pl.loop(1, fs)
    def _(k):
        f_copy(k).wait_send()
        c_copy(k).wait_send()
        n_copy(k).wait_send()

    @pl.loop(0, chunks)
    def _(c):
        x_copy(c).wait_send()
        p_copy(c).wait_send()

        @pl.loop(1, pairs)
        def _(k):
            s_copy(c, k).wait_send()


def out_kernel(gg, gl, cp, gd, rn, ogg, ogl, otg, otl, obg, obl, ogd, orn, sem):
    copies = [
        pltpu.make_async_copy(source, target, sem.at[i])
        for i, (source, target) in enumerate(((gg, ogg), (gl, ogl), (gd, ogd)))
    ]
    for copy in copies:
        copy.start()
    otg[...] = cp[0:3]
    otl[...] = cp[3:6]
    obg[...] = cp[6:7]
    obl[...] = cp[7:8]
    orn[...] = rn[...]
    for copy in copies:
        copy.wait()


def put_out(gg, gl, cp, gd, rn):
    ff = gg.shape[1]
    f32 = jnp.float32
    vmem = pl.BlockSpec(memory_space=pltpu.VMEM)
    hbm = pl.BlockSpec(memory_space=pl.ANY)
    row = jax.ShapeDtypeStruct((1, ff), f32)
    taps = jax.ShapeDtypeStruct((3, ff), f32)
    ogg, ogl, otg, otl, obg, obl, ogd, orn = pl.pallas_call(
        out_kernel,
        out_shape=(
            jax.ShapeDtypeStruct(gg.shape, gg.dtype), jax.ShapeDtypeStruct(gl.shape, gl.dtype),
            taps, taps, row, row, jax.ShapeDtypeStruct(gd.shape, gd.dtype), row),
        in_specs=[vmem] * 5,
        out_specs=(hbm, hbm, vmem, vmem, vmem, vmem, hbm, vmem),
        scratch_shapes=[pltpu.SemaphoreType.DMA((3,))],
        compiler_params=pltpu.CompilerParams(vmem_limit_bytes=2 << 20),
    )(*[pltpu.with_memory_space_constraint(value, pltpu.VMEM) for value in (gg, gl, cp, gd, rn)])
    return ogg, ogl, otg, otl, obg[0], obl[0], ogd, orn[0]


def local(
    fs, pre_gate, pre_linear, taps_gate, taps_linear, bias_gate, bias_linear, down_weight, out_grad
):
    tokens, ff = pre_gate.shape
    dc = down_weight.shape[1]
    chunk = 256
    chunks = ff // chunk
    pairs = fs // 2
    f32, bf16 = jnp.float32, jnp.bfloat16
    vmem = pl.BlockSpec(memory_space=pltpu.VMEM)
    dma = pltpu.SemaphoreType.DMA
    gg, gl, cp, gd, rn = pl.pallas_call(
        functools.partial(kernel, fs, chunk),
        out_shape=(
            pltpu.VMEM((tokens, ff), bf16),
            pltpu.VMEM((tokens, ff), bf16),
            pltpu.VMEM((8, ff), f32),
            pltpu.VMEM((ff, dc), f32),
            pltpu.VMEM((1, ff), f32),
        ),
        in_specs=[vmem] * 8,
        out_specs=(vmem,) * 5,
        scratch_shapes=[
            pltpu.VMEM((fs, ff, dc), bf16),
            pltpu.VMEM((2, pairs, ff, dc), bf16),
            pltpu.VMEM((pairs, ff, dc), bf16),
            pltpu.VMEM((pairs, ff, dc), bf16),
            pltpu.VMEM((ff, dc), f32),
            pltpu.VMEM((ff, dc), f32),
            pltpu.VMEM((fs, 8, ff), f32),
            pltpu.VMEM((8, ff), f32),
            pltpu.VMEM((8, ff), f32),
            pltpu.VMEM((fs, 1, ff), f32),
            dma((pairs,)), dma((pairs,)), dma((pairs,)), dma((pairs,)),
            dma((chunks,)), dma((chunks,)), dma((fs,)), dma((fs,)),
            dma((chunks, pairs)), dma((chunks, pairs)), dma((chunks,)), dma((chunks,)),
            dma((fs,)), dma((fs,)), dma, dma, dma((fs,)), dma((fs,)),
        ],
        compiler_params=pltpu.CompilerParams(
            collective_id=0, has_side_effects=True, vmem_limit_bytes=52 << 20),
    )(pre_gate, pre_linear, taps_gate, taps_linear, bias_gate[None], bias_linear[None],
      down_weight, out_grad)
    return put_out(gg, gl, cp, gd, rn)


def solution(mesh):
    in_specs = (
        P(("rep", "fs"), "tp"),
        P(("rep", "fs"), "tp"),
        P(None, "tp"),
        P(None, "tp"),
        P("tp"),
        P("tp"),
        P("tp", "fs"),
        P(("rep", "fs"), None),
    )
    out_specs = (
        P(("rep", "fs"), "tp"),
        P(("rep", "fs"), "tp"),
        P(None, "tp"),
        P(None, "tp"),
        P("tp"),
        P("tp"),
        P("tp", "fs"),
        P("tp"),
    )
    return jax.shard_map(
        functools.partial(local, mesh.shape["fs"]), mesh=mesh, in_specs=in_specs, out_specs=out_specs, check_vma=False)
```

```python
import functools

import jax
import jax.numpy as jnp
from jax import lax
from jax.experimental import pallas as pl
from jax.experimental.pallas import tpu as pltpu
from jax.sharding import PartitionSpec as P

MESH = pl.DeviceIdType.MESH


def shift_down(values, steps):
    if steps == 0:
        return values
    rows = lax.broadcasted_iota(jnp.int32, values.shape, 0)
    return jnp.where(rows < steps, 0.0, pltpu.roll(values, steps, 0))


def shift_up(values, steps):
    length = values.shape[0]
    rows = lax.broadcasted_iota(jnp.int32, values.shape, 0)
    return jnp.where(rows >= length - steps, 0.0, pltpu.roll(values, length - steps, 0))


def conv_chunk(values, taps, bias):
    return (
        taps[0:1] * shift_down(values, 2)
        + taps[1:2] * shift_down(values, 1)
        + taps[2:3] * values
        + bias
    )


def conv_back_chunk(grads, taps):
    return taps[0:1] * shift_up(grads, 2) + taps[1:2] * shift_up(grads, 1) + taps[2:3] * grads


def kernel(
    fs, chunk,
    pg_ref, pl_ref, tg_ref, tl_ref, bg_ref, bl_ref, w_ref, og_ref,
    gg_ref, gl_ref, cp_ref, gd_ref, rn_ref,
    wbuf, sbuf, pbuf, rbuf, xs, xr, cpbuf, cps, cpx, rnbuf,
    w_send, w_recv, y_send, y_recv, p_send, p_recv, f_send, f_recv, s_send, s_recv, x_send, x_recv,
    c_send, c_recv, cx_send, cx_recv, n_send, n_recv,
):
    me = lax.axis_index("fs")
    rep = lax.axis_index("rep")
    partner = 1 - rep
    pairs = fs // 2
    z = me // 2
    par = me % 2
    mate = me + 1 - 2 * par
    tokens, ff = pg_ref.shape
    dc = w_ref.shape[1]
    chunks = ff // chunk
    half = ff // 2
    lag = chunks // 2
    per = -(-(fs - 1) // chunks)

    def to(k):
        return lax.rem(me + k, fs)

    def rows_of(c):
        return pl.ds(pl.multiple_of(c * chunk, chunk), chunk)

    def shard(z_at, parity):
        return z_at * 2 + parity

    def z_to(k):
        return lax.rem(z + k, pairs)

    def z_from(k):
        return lax.rem(z + pairs - k, pairs)

    def my_half():
        return pl.ds(pl.multiple_of(rep * half, half), half)

    def w_copy(k):
        return pltpu.make_async_remote_copy(
            src_ref=w_ref.at[my_half()], dst_ref=wbuf.at[me, my_half()],
            send_sem=w_send.at[k], recv_sem=w_recv.at[k],
            device_id={"fs": shard(z_to(k), par)}, device_id_type=MESH)

    def y_first():
        return pltpu.make_async_remote_copy(
            src_ref=w_ref.at[my_half()], dst_ref=wbuf.at[me, my_half()],
            send_sem=y_send.at[0], recv_sem=y_recv.at[0],
            device_id={"fs": mate}, device_id_type=MESH)

    def y_copy(k):
        block = wbuf.at[shard(z_from(k), par), my_half()]
        return pltpu.make_async_remote_copy(
            src_ref=block, dst_ref=block,
            send_sem=y_send.at[k], recv_sem=y_recv.at[k],
            device_id={"fs": mate}, device_id_type=MESH)

    def f_copy(item):
        block = wbuf.at[shard(z_from(item % pairs), (par + item // pairs) % 2), my_half()]
        return pltpu.make_async_remote_copy(
            src_ref=block, dst_ref=block,
            send_sem=f_send.at[item], recv_sem=f_recv.at[item],
            device_id={"rep": partner}, device_id_type=MESH)

    def p_copy(c):
        return pltpu.make_async_remote_copy(
            src_ref=sbuf.at[1 - par, :, rows_of(c)], dst_ref=pbuf.at[:, rows_of(c)],
            send_sem=p_send.at[c], recv_sem=p_recv.at[c],
            device_id={"fs": mate}, device_id_type=MESH)

    def s_copy(c, k):
        return pltpu.make_async_remote_copy(
            src_ref=sbuf.at[par, z_to(k), rows_of(c)], dst_ref=rbuf.at[k, rows_of(c)],
            send_sem=s_send.at[c, k], recv_sem=s_recv.at[c, k],
            device_id={"fs": shard(z_to(k), par)}, device_id_type=MESH)

    def pair_sum(c):
        p_copy(c).wait_recv()
        for at in range(pairs):
            both = sbuf[par, at, rows_of(c)].astype(jnp.float32) + pbuf[at, rows_of(c)].astype(jnp.float32)
            sbuf[par, at, rows_of(c)] = both.astype(jnp.bfloat16)

        @pl.loop(1, pairs)
        def _(k):
            s_copy(c, k).start()

    def x_copy(c):
        return pltpu.make_async_remote_copy(
            src_ref=xs.at[rows_of(c)], dst_ref=xr.at[rows_of(c)],
            send_sem=x_send.at[c], recv_sem=x_recv.at[c],
            device_id={"rep": partner}, device_id_type=MESH)

    def c_copy(k):
        return pltpu.make_async_remote_copy(
            src_ref=cpbuf.at[me], dst_ref=cpbuf.at[me],
            send_sem=c_send.at[k], recv_sem=c_recv.at[k],
            device_id={"fs": to(k)}, device_id_type=MESH)

    def cx_copy():
        return pltpu.make_async_remote_copy(
            src_ref=cps, dst_ref=cpx, send_sem=cx_send, recv_sem=cx_recv,
            device_id={"rep": partner}, device_id_type=MESH)

    def n_copy(k):
        return pltpu.make_async_remote_copy(
            src_ref=rnbuf.at[me], dst_ref=rnbuf.at[me],
            send_sem=n_send.at[k], recv_sem=n_recv.at[k],
            device_id={"fs": to(k)}, device_id_type=MESH)

    barrier = pltpu.get_barrier_semaphore()

    @pl.loop(1, fs)
    def _(k):
        pl.semaphore_signal(barrier, inc=1, device_id={"fs": to(k)}, device_id_type=MESH)

    pl.semaphore_signal(barrier, inc=1, device_id={"rep": partner}, device_id_type=MESH)
    pl.semaphore_wait(barrier, fs)

    y_first().start()

    @pl.loop(1, pairs)
    def _(k):
        w_copy(k).start()

    wbuf[me] = w_ref[...]

    @pl.loop(0, chunks)
    def _(c):
        cols = rows_of(c)
        gate_pre = conv_chunk(
            pg_ref[:, cols].astype(jnp.float32), tg_ref[:, cols], bg_ref[:, cols])
        linear_pre = conv_chunk(
            pl_ref[:, cols].astype(jnp.float32), tl_ref[:, cols], bl_ref[:, cols])
        hidden = (gate_pre * jax.nn.sigmoid(gate_pre) * linear_pre).astype(jnp.bfloat16)
        for j in range(fs):
            part = lax.dot_general(
                hidden, og_ref[:, j * dc:(j + 1) * dc], (((0,), (0,)), ((), ())),
                preferred_element_type=jnp.float32)
            sbuf[j % 2, j // 2, cols] = part.astype(jnp.bfloat16)

        p_copy(c).start()

        @pl.when(c >= lag)
        def _():
            pair_sum(c - lag)

        for step in range(per):
            k = c * per + step + 1

            @pl.when(k < pairs)
            def _():
                w_copy(k).wait_recv()
                y_copy(k).start()
                f_copy(k).start()

            @pl.when((k >= pairs) & (k < fs))
            def _():
                y_copy(k - pairs).wait_recv()
                f_copy(k).start()

    @pl.loop(1, fs)
    def _(k):
        f_copy(k).wait_recv()

    @pl.loop(0, chunks)
    def _(c):
        cols = rows_of(c)
        gate_in = pg_ref[:, cols].astype(jnp.float32)
        linear_in = pl_ref[:, cols].astype(jnp.float32)
        taps_gate, taps_linear = tg_ref[:, cols], tl_ref[:, cols]
        gate_pre = conv_chunk(gate_in, taps_gate, bg_ref[:, cols])
        linear_pre = conv_chunk(linear_in, taps_linear, bl_ref[:, cols])
        sigma = jax.nn.sigmoid(gate_pre)
        grad_hidden = jnp.zeros((tokens, chunk), jnp.float32)
        for j in range(fs):
            grad_hidden += lax.dot_general(
                og_ref[:, j * dc:(j + 1) * dc], wbuf[j, cols], (((1,), (1,)), ((), ())),
                preferred_element_type=jnp.float32)
        grad_gate_pre = grad_hidden * linear_pre * sigma * (1.0 + gate_pre * (1.0 - sigma))
        grad_linear_pre = grad_hidden * (gate_pre * sigma)
        gg_ref[:, cols] = conv_back_chunk(grad_gate_pre, taps_gate).astype(jnp.bfloat16)
        gl_ref[:, cols] = conv_back_chunk(grad_linear_pre, taps_linear).astype(jnp.bfloat16)
        for j in range(3):
            cpbuf[me, j:j + 1, cols] = jnp.sum(
                grad_gate_pre * shift_down(gate_in, 2 - j), axis=0, keepdims=True)
            cpbuf[me, j + 3:j + 4, cols] = jnp.sum(
                grad_linear_pre * shift_down(linear_in, 2 - j), axis=0, keepdims=True)
        cpbuf[me, 6:7, cols] = jnp.sum(grad_gate_pre, axis=0, keepdims=True)
        cpbuf[me, 7:8, cols] = jnp.sum(grad_linear_pre, axis=0, keepdims=True)

        @pl.when(c == chunks - 1)
        def _():
            @pl.loop(1, fs)
            def _(k):
                c_copy(k).start()

        @pl.when(c < lag)
        def _():
            pair_sum(chunks - lag + c)

        total = sbuf[par, z, cols].astype(jnp.float32)
        for k in range(1, pairs):
            s_copy(c, k).wait_recv()
            total += rbuf[k, cols].astype(jnp.float32)
        xs[cols] = total
        x_copy(c).start()

    @pl.loop(1, fs)
    def _(k):
        c_copy(k).wait_recv()

    sums = cpbuf[0]
    for j in range(1, fs):
        sums += cpbuf[j]
    cps[...] = sums
    cx_copy().start()

    @pl.loop(0, chunks)
    def _(c):
        rows = rows_of(c)
        x_copy(c).wait_recv()
        total = xs[rows] + xr[rows]
        gd_ref[rows] = total
        square = total * total
        while square.shape[1] % 256 == 0:
            middle = square.shape[1] // 2
            square = square[:, :middle] + square[:, middle:]
        rnbuf[me, 0:1, rows] = jnp.sum(square.T, axis=0, keepdims=True)

    @pl.loop(1, fs)
    def _(k):
        n_copy(k).start()

    cx_copy().wait_recv()
    cp_ref[...] = cps[...] + cpx[...]

    @pl.loop(1, fs)
    def _(k):
        n_copy(k).wait_recv()

    norms = rnbuf[0]
    for j in range(1, fs):
        norms += rnbuf[j]
    rn_ref[...] = norms

    cx_copy().wait_send()
    y_first().wait_send()

    @pl.loop(1, pairs)
    def _(k):
        w_copy(k).wait_send()
        y_copy(k).wait_send()

    @pl.loop(1, fs)
    def _(k):
        f_copy(k).wait_send()
        c_copy(k).wait_send()
        n_copy(k).wait_send()

    @pl.loop(0, chunks)
    def _(c):
        x_copy(c).wait_send()
        p_copy(c).wait_send()

        @pl.loop(1, pairs)
        def _(k):
            s_copy(c, k).wait_send()


def out_kernel(gg, gl, cp, gd, rn, ogg, ogl, otg, otl, obg, obl, ogd, orn, sem):
    copies = [
        pltpu.make_async_copy(source, target, sem.at[i])
        for i, (source, target) in enumerate(((gg, ogg), (gl, ogl), (gd, ogd)))
    ]
    for copy in copies:
        copy.start()
    otg[...] = cp[0:3]
    otl[...] = cp[3:6]
    obg[...] = cp[6:7]
    obl[...] = cp[7:8]
    width = rn.shape[1]
    for i in range(rn.shape[0]):
        orn[0:1, i * width:(i + 1) * width] = rn[i:i + 1]
    for copy in copies:
        copy.wait()


def put_out(gg, gl, cp, gd, rn):
    ff = gg.shape[1]
    f32 = jnp.float32
    vmem = pl.BlockSpec(memory_space=pltpu.VMEM)
    hbm = pl.BlockSpec(memory_space=pl.ANY)
    row = jax.ShapeDtypeStruct((1, ff), f32)
    taps = jax.ShapeDtypeStruct((3, ff), f32)
    ogg, ogl, otg, otl, obg, obl, ogd, orn = pl.pallas_call(
        out_kernel,
        out_shape=(
            jax.ShapeDtypeStruct(gg.shape, gg.dtype), jax.ShapeDtypeStruct(gl.shape, gl.dtype),
            taps, taps, row, row, jax.ShapeDtypeStruct(gd.shape, gd.dtype), row),
        in_specs=[vmem] * 5,
        out_specs=(hbm, hbm, vmem, vmem, vmem, vmem, hbm, vmem),
        scratch_shapes=[pltpu.SemaphoreType.DMA((3,))],
        compiler_params=pltpu.CompilerParams(vmem_limit_bytes=2 << 20),
    )(*[pltpu.with_memory_space_constraint(value, pltpu.VMEM) for value in (gg, gl, cp, gd, rn)])
    return ogg, ogl, otg, otl, obg[0], obl[0], ogd, orn[0]


def direct_local(
    fs, pre_gate, pre_linear, taps_gate, taps_linear, bias_gate, bias_linear, down_weight, out_grad
):
    tokens, ff = pre_gate.shape
    dc = down_weight.shape[1]
    chunk = 256
    chunks = ff // chunk
    pairs = fs // 2
    f32, bf16 = jnp.float32, jnp.bfloat16
    vmem = pl.BlockSpec(memory_space=pltpu.VMEM)
    dma = pltpu.SemaphoreType.DMA
    gg, gl, cp, gd, rn = pl.pallas_call(
        functools.partial(kernel, fs, chunk),
        out_shape=(
            pltpu.VMEM((tokens, ff), bf16),
            pltpu.VMEM((tokens, ff), bf16),
            pltpu.VMEM((8, ff), f32),
            pltpu.VMEM((ff, dc), f32),
            pltpu.VMEM((1, ff), f32),
        ),
        in_specs=[vmem] * 8,
        out_specs=(vmem,) * 5,
        scratch_shapes=[
            pltpu.VMEM((fs, ff, dc), bf16),
            pltpu.VMEM((2, pairs, ff, dc), bf16),
            pltpu.VMEM((pairs, ff, dc), bf16),
            pltpu.VMEM((pairs, ff, dc), bf16),
            pltpu.VMEM((ff, dc), f32),
            pltpu.VMEM((ff, dc), f32),
            pltpu.VMEM((fs, 8, ff), f32),
            pltpu.VMEM((8, ff), f32),
            pltpu.VMEM((8, ff), f32),
            pltpu.VMEM((fs, 1, ff), f32),
            dma((pairs,)), dma((pairs,)), dma((pairs,)), dma((pairs,)),
            dma((chunks,)), dma((chunks,)), dma((fs,)), dma((fs,)),
            dma((chunks, pairs)), dma((chunks, pairs)), dma((chunks,)), dma((chunks,)),
            dma((fs,)), dma((fs,)), dma, dma, dma((fs,)), dma((fs,)),
        ],
        compiler_params=pltpu.CompilerParams(
            collective_id=0, has_side_effects=True, vmem_limit_bytes=52 << 20),
    )(pre_gate, pre_linear, taps_gate, taps_linear, bias_gate[None], bias_linear[None],
      down_weight, out_grad)
    return put_out(gg, gl, cp, gd, rn)


def line_kernel(
    fs, unit,
    pg_hbm, pl_hbm, tg_ref, tl_ref, bg_ref, bl_ref, w_hbm, og_hbm,
    gg_ref, gl_ref, cp_ref, gd_ref, rn_ref,
    og, pg, pln, wbuf, xs, xr, own, zb, ys, yr, cpl, cpr, cps, rnb,
    in_sem, og_sem, w_sem, x_send, x_recv, wz_send, wz_recv, wy_send, wy_recv,
    zu_send, zu_recv, zd_send, zd_recv, y_send, y_recv, a_send, a_recv,
    c_send, c_recv, b_send, b_recv, n_send, n_recv,
):
    me = lax.axis_index("fs")
    rep = lax.axis_index("rep")
    partner = 1 - rep
    nz = fs // 2
    peers = 2 * fs
    z = me // 2
    y = me % 2
    mate = me + 1 - 2 * y
    flat = rep * fs + me
    tokens, ff = pg_hbm.shape
    dc = w_hbm.shape[1]
    units = ff // unit
    half = unit // 2
    chunks = 2 * units
    ch = half // 2
    span = ff // peers
    wch = unit // 2

    def unit_cols(u):
        return pl.ds(pl.multiple_of(u * unit, unit), unit)

    def half_cols(u, side):
        return pl.ds(pl.multiple_of(u * unit + side * half, half), half)

    def chunk_rows(c, side):
        start = (c // 2) * unit + side * half + (c % 2) * ch
        return pl.ds(pl.multiple_of(start, ch), ch)

    def w_rows(k):
        return pl.ds(pl.multiple_of(k * wch, wch), wch)

    def peer(k):
        at = lax.rem(flat + k, peers)
        return {"rep": at // fs, "fs": at % fs}

    def remote(source, target, send, recv, device):
        return pltpu.make_async_remote_copy(
            src_ref=source, dst_ref=target, send_sem=send, recv_sem=recv,
            device_id=device, device_id_type=MESH)

    def in_copies(u):
        cols = unit_cols(u)
        return (
            pltpu.make_async_copy(pg_hbm.at[:, cols], pg.at[:, cols], in_sem.at[0, u]),
            pltpu.make_async_copy(pl_hbm.at[:, cols], pln.at[:, cols], in_sem.at[1, u]))

    def og_copy():
        return pltpu.make_async_copy(og_hbm, og, og_sem)

    def w_copy():
        return pltpu.make_async_copy(w_hbm, wbuf.at[me], w_sem)

    def x_copy(c):
        return remote(xs.at[c], xr.at[c], x_send.at[c], x_recv.at[c], {"rep": partner})

    def wz_copy(way, k, src):
        block = wbuf.at[src * 2 + y, w_rows(k)]
        to = z + 1 if way == 0 else z - 1
        return remote(block, block, wz_send.at[way, k, src], wz_recv.at[k, src], {"fs": to * 2 + y})

    def wy_copy(k, src):
        block = wbuf.at[src * 2 + y, w_rows(k)]
        return remote(block, block, wy_send.at[k, src], wy_recv.at[k, src], {"fs": mate})

    def z_up(c, i):
        return remote(
            zb.at[c, i], zb.at[c, i], zu_send.at[c, i], zu_recv.at[c, i], {"fs": (z + 1) * 2 + y})

    def z_down(c, i):
        slot = jnp.where(i == z - 1, nz, i)
        return remote(
            zb.at[c, i], zb.at[c, slot], zd_send.at[c, i], zd_recv.at[c, i], {"fs": (z - 1) * 2 + y})

    def y_copy(c):
        return remote(ys.at[c], yr.at[c], y_send.at[c], y_recv.at[c], {"fs": mate})

    def a_copy(c):
        rows = chunk_rows(c, rep)
        return remote(gd_ref.at[rows], gd_ref.at[rows], a_send.at[c], a_recv.at[c], {"rep": partner})

    def c_copy(k):
        at = lax.rem(flat + k, peers)
        cols = pl.ds(pl.multiple_of(at * span, span), span)
        return remote(cpl.at[:, cols], cpr.at[flat], c_send.at[k], c_recv.at[k], peer(k))

    def my_span():
        return pl.ds(pl.multiple_of(flat * span, span), span)

    def b_copy(k):
        return remote(cps, cp_ref.at[:, my_span()], b_send.at[k], b_recv.at[k], peer(k))

    def n_copy(k):
        return remote(rnb.at[flat], rnb.at[flat], n_send.at[k], n_recv.at[k], peer(k))

    barrier = pltpu.get_barrier_semaphore()

    @pl.loop(1, peers)
    def _(k):
        pl.semaphore_signal(barrier, inc=1, device_id=peer(k), device_id_type=MESH)

    w_copy().start()
    for copy in in_copies(0):
        copy.start()
    og_copy().start()

    @pl.loop(1, units)
    def _(u):
        for copy in in_copies(u):
            copy.start()

    w_copy().wait()
    pl.semaphore_wait(barrier, peers - 1)

    def hidden_half(cols):
        gate_pre = conv_chunk(pg[:, cols].astype(jnp.float32), tg_ref[:, cols], bg_ref[:, cols])
        linear_pre = conv_chunk(pln[:, cols].astype(jnp.float32), tl_ref[:, cols], bl_ref[:, cols])
        return (gate_pre * jax.nn.sigmoid(gate_pre) * linear_pre).astype(jnp.bfloat16)

    def forward(u):
        for copy in in_copies(u):
            copy.wait()
        hidden = jnp.concatenate(
            [hidden_half(half_cols(u, rep)), hidden_half(half_cols(u, partner))], axis=1)
        for j in range(fs):
            part = lax.dot_general(
                hidden, og[:, j * dc:(j + 1) * dc], (((0,), (0,)), ((), ())),
                preferred_element_type=jnp.float32)
            for h in range(2):
                own[2 * u + h, j // 2, j % 2] = part[h * ch:(h + 1) * ch]
                xs[2 * u + h, j // 2, j % 2] = part[half + h * ch:half + (h + 1) * ch].astype(jnp.bfloat16)
        x_copy(2 * u).start()
        x_copy(2 * u + 1).start()

    def backward(u):
        cols = unit_cols(u)
        for k in range(2):
            for src in range(nz):
                wy_copy(2 * u + k, src).wait_recv()
        gate_in = pg[:, cols].astype(jnp.float32)
        linear_in = pln[:, cols].astype(jnp.float32)
        taps_gate, taps_linear = tg_ref[:, cols], tl_ref[:, cols]
        gate_pre = conv_chunk(gate_in, taps_gate, bg_ref[:, cols])
        linear_pre = conv_chunk(linear_in, taps_linear, bl_ref[:, cols])
        sigma = jax.nn.sigmoid(gate_pre)
        grad_hidden = jnp.zeros((tokens, unit), jnp.float32)
        for j in range(fs):
            grad_hidden += lax.dot_general(
                og[:, j * dc:(j + 1) * dc], wbuf[j, cols], (((1,), (1,)), ((), ())),
                preferred_element_type=jnp.float32)
        grad_gate_pre = grad_hidden * linear_pre * sigma * (1.0 + gate_pre * (1.0 - sigma))
        grad_linear_pre = grad_hidden * (gate_pre * sigma)
        gg_ref[:, cols] = conv_back_chunk(grad_gate_pre, taps_gate).astype(jnp.bfloat16)
        gl_ref[:, cols] = conv_back_chunk(grad_linear_pre, taps_linear).astype(jnp.bfloat16)
        for j in range(3):
            cpl[j:j + 1, cols] = jnp.sum(
                grad_gate_pre * shift_down(gate_in, 2 - j), axis=0, keepdims=True)
            cpl[j + 3:j + 4, cols] = jnp.sum(
                grad_linear_pre * shift_down(linear_in, 2 - j), axis=0, keepdims=True)
        cpl[6:7, cols] = jnp.sum(grad_gate_pre, axis=0, keepdims=True)
        cpl[7:8, cols] = jnp.sum(grad_linear_pre, axis=0, keepdims=True)
        count = unit // span
        for b in range(count):
            k = lax.rem(u * count + b - flat + peers, peers)

            @pl.when(k != 0)
            def _():
                c_copy(k).start()

    def weights(t):
        @pl.when(t < chunks)
        def _():
            @pl.when(z < nz - 1)
            def _():
                wz_copy(0, t, z).start()

            @pl.when(z > 0)
            def _():
                wz_copy(1, t, z).start()

            wy_copy(t, z).start()

        for d in range(1, nz):
            k = t - d
            live = (k >= 0) & (k < chunks)

            @pl.when(live & (z >= d))
            def _():
                wz_copy(0, k, z - d).wait_recv()

                @pl.when(z < nz - 1)
                def _():
                    wz_copy(0, k, z - d).start()

                wy_copy(k, z - d).start()

            @pl.when(live & (z + d < nz))
            def _():
                wz_copy(1, k, z + d).wait_recv()

                @pl.when(z > 0)
                def _():
                    wz_copy(1, k, z + d).start()

                wy_copy(k, z + d).start()

    def add_step(c, s):
        up = z + nz - s
        down = z - nz + s

        @pl.when(z <= s - 1)
        def _():
            total = own[c, up] + xr[c, up].astype(jnp.float32)

            @pl.when(z > 0)
            def _():
                z_up(c, up).wait_recv()
                zb[c, up] = (total + zb[c, up].astype(jnp.float32)).astype(jnp.bfloat16)

            @pl.when(z == 0)
            def _():
                zb[c, up] = total.astype(jnp.bfloat16)

            z_up(c, up).start()

        @pl.when(z >= nz - s)
        def _():
            total = own[c, down] + xr[c, down].astype(jnp.float32)

            @pl.when(z < nz - 1)
            def _():
                z_down(c, down).wait_recv()
                zb[c, down] = (total + zb[c, down].astype(jnp.float32)).astype(jnp.bfloat16)

            @pl.when(z == nz - 1)
            def _():
                zb[c, down] = total.astype(jnp.bfloat16)

            z_down(c, down).start()

    def line_end(c):
        own[c, z] += xr[c, z].astype(jnp.float32)

        @pl.when(z > 0)
        def _():
            z_up(c, z).wait_recv()
            own[c, z] += zb[c, z].astype(jnp.float32)

        @pl.when(z < nz - 1)
        def _():
            z_down(c, z).wait_recv()
            own[c, z] += zb[c, nz].astype(jnp.float32)

        ys[c] = own[c, z, 1 - y].astype(jnp.bfloat16)
        y_copy(c).start()

    def finish(c):
        y_copy(c).wait_recv()
        gd_ref[chunk_rows(c, rep)] = own[c, z, y] + yr[c].astype(jnp.float32)
        a_copy(c).start()

        @pl.when(c % 2 == 1)
        def _():
            u = c // 2
            total = gd_ref[half_cols(u, rep)]
            square = total * total
            while square.shape[1] % 256 == 0:
                middle = square.shape[1] // 2
                square = square[:, :middle] + square[:, middle:]
            rnb[flat, pl.ds(u, 1)] = jnp.sum(square.T, axis=0, keepdims=True)

    ticks = chunks + nz + 1

    @pl.loop(0, ticks)
    def _(t):
        weights(t)

        c = t - 1 - nz

        @pl.when((c >= 0) & (c < chunks))
        def _():
            finish(c)

        c = t - nz

        @pl.when((c >= 0) & (c < chunks))
        def _():
            line_end(c)

        for s in range(nz - 1, 0, -1):
            c = t - s

            @pl.when((c >= 0) & (c < chunks))
            def _():
                if s == 1:
                    x_copy(c).wait_recv()
                add_step(c, s)

        @pl.when(t < units)
        def _():
            @pl.when(t == 0)
            def _():
                og_copy().wait()

            forward(t)

        late = t - nz - 1

        @pl.when((late >= 0) & (late % 2 == 0) & (late < chunks))
        def _():
            backward(late // 2)

    @pl.loop(1, peers)
    def _(k):
        n_copy(k).start()

    cpr[flat] = cpl[:, my_span()]

    @pl.loop(1, peers)
    def _(k):
        c_copy(k).wait_recv()

    sums = cpr[0]
    for j in range(1, peers):
        sums += cpr[j]
    cps[...] = sums
    cp_ref[:, my_span()] = sums

    @pl.loop(1, peers)
    def _(k):
        b_copy(k).start()

    @pl.loop(1, peers)
    def _(k):
        n_copy(k).wait_recv()

    for side in range(2):
        norms = rnb[side * fs]
        for j in range(1, fs):
            norms += rnb[side * fs + j]
        rn_ref[:, side * half:(side + 1) * half] = norms

    @pl.loop(1, peers)
    def _(k):
        b_copy(k).wait_recv()

    @pl.loop(0, chunks)
    def _(c):
        a_copy(c).wait_recv()

    @pl.loop(1, peers)
    def _(k):
        n_copy(k).wait_send()
        c_copy(k).wait_send()
        b_copy(k).wait_send()

    @pl.loop(0, chunks)
    def _(c):
        x_copy(c).wait_send()
        y_copy(c).wait_send()
        a_copy(c).wait_send()

        @pl.loop(0, nz)
        def _(i):
            @pl.when(i > z)
            def _():
                z_up(c, i).wait_send()

            @pl.when(i < z)
            def _():
                z_down(c, i).wait_send()

            wy_copy(c, i).wait_send()

            @pl.when((i <= z) & (z < nz - 1))
            def _():
                wz_copy(0, c, i).wait_send()

            @pl.when((i >= z) & (z > 0))
            def _():
                wz_copy(1, c, i).wait_send()


def line_local(
    fs, pre_gate, pre_linear, taps_gate, taps_linear, bias_gate, bias_linear, down_weight, out_grad
):
    tokens, ff = pre_gate.shape
    dc = down_weight.shape[1]
    unit = 256
    units = ff // unit
    chunks = 2 * units
    ch = unit // 4
    nz = fs // 2
    peers = 2 * fs
    f32, bf16 = jnp.float32, jnp.bfloat16
    vmem = pl.BlockSpec(memory_space=pltpu.VMEM)
    hbm = pl.BlockSpec(memory_space=pl.ANY)
    dma = pltpu.SemaphoreType.DMA
    gg, gl, cp, gd, rn = pl.pallas_call(
        functools.partial(line_kernel, fs, unit),
        out_shape=(
            pltpu.VMEM((tokens, ff), bf16),
            pltpu.VMEM((tokens, ff), bf16),
            pltpu.VMEM((8, ff), f32),
            pltpu.VMEM((ff, dc), f32),
            pltpu.VMEM((units, unit), f32),
        ),
        in_specs=[hbm, hbm, vmem, vmem, vmem, vmem, hbm, hbm],
        out_specs=(vmem,) * 5,
        scratch_shapes=[
            pltpu.VMEM((tokens, out_grad.shape[1]), bf16),
            pltpu.VMEM((tokens, ff), bf16),
            pltpu.VMEM((tokens, ff), bf16),
            pltpu.VMEM((fs, ff, dc), bf16),
            pltpu.VMEM((chunks, nz, 2, ch, dc), bf16),
            pltpu.VMEM((chunks, nz, 2, ch, dc), bf16),
            pltpu.VMEM((chunks, nz, 2, ch, dc), f32),
            pltpu.VMEM((chunks, nz + 1, 2, ch, dc), bf16),
            pltpu.VMEM((chunks, ch, dc), bf16),
            pltpu.VMEM((chunks, ch, dc), bf16),
            pltpu.VMEM((8, ff), f32),
            pltpu.VMEM((peers, 8, ff // peers), f32),
            pltpu.VMEM((8, ff // peers), f32),
            pltpu.VMEM((peers, units, unit // 2), f32),
            dma((2, units)), dma, dma,
            dma((chunks,)), dma((chunks,)),
            dma((2, chunks, nz)), dma((chunks, nz)), dma((chunks, nz)), dma((chunks, nz)),
            dma((chunks, nz)), dma((chunks, nz)), dma((chunks, nz)), dma((chunks, nz)),
            dma((chunks,)), dma((chunks,)), dma((chunks,)), dma((chunks,)),
            dma((peers,)), dma((peers,)), dma((peers,)), dma((peers,)), dma((peers,)), dma((peers,)),
        ],
        compiler_params=pltpu.CompilerParams(
            collective_id=0, has_side_effects=True, vmem_limit_bytes=55 << 20),
    )(pre_gate, pre_linear, taps_gate, taps_linear, bias_gate[None], bias_linear[None],
      down_weight, out_grad)
    return put_out(gg, gl, cp, gd, rn)


def on_a_line(fs, ff, dc):
    nz = fs // 2
    return fs % 2 == 0 and 2 <= nz <= 4 and ff % (256 * fs) == 0 and dc % 128 == 0


def local(fs, *args):
    if on_a_line(fs, args[0].shape[1], args[6].shape[1]):
        return line_local(fs, *args)
    return direct_local(fs, *args)


def solution(mesh):
    in_specs = (
        P(("rep", "fs"), "tp"),
        P(("rep", "fs"), "tp"),
        P(None, "tp"),
        P(None, "tp"),
        P("tp"),
        P("tp"),
        P("tp", "fs"),
        P(("rep", "fs"), None),
    )
    out_specs = (
        P(("rep", "fs"), "tp"),
        P(("rep", "fs"), "tp"),
        P(None, "tp"),
        P(None, "tp"),
        P("tp"),
        P("tp"),
        P("tp", "fs"),
        P("tp"),
    )
    return jax.shard_map(
        functools.partial(local, mesh.shape["fs"]), mesh=mesh, in_specs=in_specs, out_specs=out_specs, check_vma=False)
```

```python
import functools

import jax
import jax.numpy as jnp
from jax import lax
from jax.experimental import pallas as pl
from jax.experimental.pallas import tpu as pltpu
from jax.sharding import PartitionSpec as P

MESH = pl.DeviceIdType.MESH


def shift_down(values, steps):
    if steps == 0:
        return values
    rows = lax.broadcasted_iota(jnp.int32, values.shape, 0)
    return jnp.where(rows < steps, 0.0, pltpu.roll(values, steps, 0))


def shift_up(values, steps):
    length = values.shape[0]
    rows = lax.broadcasted_iota(jnp.int32, values.shape, 0)
    return jnp.where(rows >= length - steps, 0.0, pltpu.roll(values, length - steps, 0))


def conv_chunk(values, taps, bias):
    return (
        taps[0:1] * shift_down(values, 2)
        + taps[1:2] * shift_down(values, 1)
        + taps[2:3] * values
        + bias
    )


def conv_back_chunk(grads, taps):
    return taps[0:1] * shift_up(grads, 2) + taps[1:2] * shift_up(grads, 1) + taps[2:3] * grads


def kernel(
    fs, chunk,
    pg_ref, pl_ref, tg_ref, tl_ref, bg_ref, bl_ref, w_ref, og_ref,
    gg_ref, gl_ref, cp_ref, gd_ref, rn_ref,
    wbuf, sbuf, pbuf, rbuf, xs, xr, cpbuf, cps, cpx, rnbuf,
    w_send, w_recv, y_send, y_recv, p_send, p_recv, f_send, f_recv, s_send, s_recv, x_send, x_recv,
    c_send, c_recv, cx_send, cx_recv, n_send, n_recv,
):
    me = lax.axis_index("fs")
    rep = lax.axis_index("rep")
    partner = 1 - rep
    pairs = fs // 2
    z = me // 2
    par = me % 2
    mate = me + 1 - 2 * par
    tokens, ff = pg_ref.shape
    dc = w_ref.shape[1]
    chunks = ff // chunk
    half = ff // 2
    lag = chunks // 2
    per = -(-(fs - 1) // chunks)

    def to(k):
        return lax.rem(me + k, fs)

    def rows_of(c):
        return pl.ds(pl.multiple_of(c * chunk, chunk), chunk)

    def shard(z_at, parity):
        return z_at * 2 + parity

    def z_to(k):
        return lax.rem(z + k, pairs)

    def z_from(k):
        return lax.rem(z + pairs - k, pairs)

    def my_half():
        return pl.ds(pl.multiple_of(rep * half, half), half)

    def w_copy(k):
        return pltpu.make_async_remote_copy(
            src_ref=w_ref.at[my_half()], dst_ref=wbuf.at[me, my_half()],
            send_sem=w_send.at[k], recv_sem=w_recv.at[k],
            device_id={"fs": shard(z_to(k), par)}, device_id_type=MESH)

    def y_first():
        return pltpu.make_async_remote_copy(
            src_ref=w_ref.at[my_half()], dst_ref=wbuf.at[me, my_half()],
            send_sem=y_send.at[0], recv_sem=y_recv.at[0],
            device_id={"fs": mate}, device_id_type=MESH)

    def y_copy(k):
        block = wbuf.at[shard(z_from(k), par), my_half()]
        return pltpu.make_async_remote_copy(
            src_ref=block, dst_ref=block,
            send_sem=y_send.at[k], recv_sem=y_recv.at[k],
            device_id={"fs": mate}, device_id_type=MESH)

    def f_copy(item):
        block = wbuf.at[shard(z_from(item % pairs), (par + item // pairs) % 2), my_half()]
        return pltpu.make_async_remote_copy(
            src_ref=block, dst_ref=block,
            send_sem=f_send.at[item], recv_sem=f_recv.at[item],
            device_id={"rep": partner}, device_id_type=MESH)

    def p_copy(c):
        return pltpu.make_async_remote_copy(
            src_ref=sbuf.at[1 - par, :, rows_of(c)], dst_ref=pbuf.at[:, rows_of(c)],
            send_sem=p_send.at[c], recv_sem=p_recv.at[c],
            device_id={"fs": mate}, device_id_type=MESH)

    def s_copy(c, k):
        return pltpu.make_async_remote_copy(
            src_ref=sbuf.at[par, z_to(k), rows_of(c)], dst_ref=rbuf.at[k, rows_of(c)],
            send_sem=s_send.at[c, k], recv_sem=s_recv.at[c, k],
            device_id={"fs": shard(z_to(k), par)}, device_id_type=MESH)

    def pair_sum(c):
        p_copy(c).wait_recv()
        for at in range(pairs):
            both = sbuf[par, at, rows_of(c)].astype(jnp.float32) + pbuf[at, rows_of(c)].astype(jnp.float32)
            sbuf[par, at, rows_of(c)] = both.astype(jnp.bfloat16)

        @pl.loop(1, pairs)
        def _(k):
            s_copy(c, k).start()

    def x_copy(c):
        return pltpu.make_async_remote_copy(
            src_ref=xs.at[rows_of(c)], dst_ref=xr.at[rows_of(c)],
            send_sem=x_send.at[c], recv_sem=x_recv.at[c],
            device_id={"rep": partner}, device_id_type=MESH)

    def c_copy(k):
        return pltpu.make_async_remote_copy(
            src_ref=cpbuf.at[me], dst_ref=cpbuf.at[me],
            send_sem=c_send.at[k], recv_sem=c_recv.at[k],
            device_id={"fs": to(k)}, device_id_type=MESH)

    def cx_copy():
        return pltpu.make_async_remote_copy(
            src_ref=cps, dst_ref=cpx, send_sem=cx_send, recv_sem=cx_recv,
            device_id={"rep": partner}, device_id_type=MESH)

    def n_copy(k):
        return pltpu.make_async_remote_copy(
            src_ref=rnbuf.at[me], dst_ref=rnbuf.at[me],
            send_sem=n_send.at[k], recv_sem=n_recv.at[k],
            device_id={"fs": to(k)}, device_id_type=MESH)

    barrier = pltpu.get_barrier_semaphore()

    @pl.loop(1, fs)
    def _(k):
        pl.semaphore_signal(barrier, inc=1, device_id={"fs": to(k)}, device_id_type=MESH)

    pl.semaphore_signal(barrier, inc=1, device_id={"rep": partner}, device_id_type=MESH)
    pl.semaphore_wait(barrier, fs)

    y_first().start()

    @pl.loop(1, pairs)
    def _(k):
        w_copy(k).start()

    wbuf[me] = w_ref[...]

    @pl.loop(0, chunks)
    def _(c):
        cols = rows_of(c)
        gate_pre = conv_chunk(
            pg_ref[:, cols].astype(jnp.float32), tg_ref[:, cols], bg_ref[:, cols])
        linear_pre = conv_chunk(
            pl_ref[:, cols].astype(jnp.float32), tl_ref[:, cols], bl_ref[:, cols])
        hidden = (gate_pre * jax.nn.sigmoid(gate_pre) * linear_pre).astype(jnp.bfloat16)
        for j in range(fs):
            part = lax.dot_general(
                hidden, og_ref[:, j * dc:(j + 1) * dc], (((0,), (0,)), ((), ())),
                preferred_element_type=jnp.float32)
            sbuf[j % 2, j // 2, cols] = part.astype(jnp.bfloat16)

        p_copy(c).start()

        @pl.when(c >= lag)
        def _():
            pair_sum(c - lag)

        for step in range(per):
            k = c * per + step + 1

            @pl.when(k < pairs)
            def _():
                w_copy(k).wait_recv()
                y_copy(k).start()
                f_copy(k).start()

            @pl.when((k >= pairs) & (k < fs))
            def _():
                y_copy(k - pairs).wait_recv()
                f_copy(k).start()

    @pl.loop(1, fs)
    def _(k):
        f_copy(k).wait_recv()

    @pl.loop(0, chunks)
    def _(c):
        cols = rows_of(c)
        gate_in = pg_ref[:, cols].astype(jnp.float32)
        linear_in = pl_ref[:, cols].astype(jnp.float32)
        taps_gate, taps_linear = tg_ref[:, cols], tl_ref[:, cols]
        gate_pre = conv_chunk(gate_in, taps_gate, bg_ref[:, cols])
        linear_pre = conv_chunk(linear_in, taps_linear, bl_ref[:, cols])
        sigma = jax.nn.sigmoid(gate_pre)
        grad_hidden = jnp.zeros((tokens, chunk), jnp.float32)
        for j in range(fs):
            grad_hidden += lax.dot_general(
                og_ref[:, j * dc:(j + 1) * dc], wbuf[j, cols], (((1,), (1,)), ((), ())),
                preferred_element_type=jnp.float32)
        grad_gate_pre = grad_hidden * linear_pre * sigma * (1.0 + gate_pre * (1.0 - sigma))
        grad_linear_pre = grad_hidden * (gate_pre * sigma)
        gg_ref[:, cols] = conv_back_chunk(grad_gate_pre, taps_gate).astype(jnp.bfloat16)
        gl_ref[:, cols] = conv_back_chunk(grad_linear_pre, taps_linear).astype(jnp.bfloat16)
        for j in range(3):
            cpbuf[me, j:j + 1, cols] = jnp.sum(
                grad_gate_pre * shift_down(gate_in, 2 - j), axis=0, keepdims=True)
            cpbuf[me, j + 3:j + 4, cols] = jnp.sum(
                grad_linear_pre * shift_down(linear_in, 2 - j), axis=0, keepdims=True)
        cpbuf[me, 6:7, cols] = jnp.sum(grad_gate_pre, axis=0, keepdims=True)
        cpbuf[me, 7:8, cols] = jnp.sum(grad_linear_pre, axis=0, keepdims=True)

        @pl.when(c == chunks - 1)
        def _():
            @pl.loop(1, fs)
            def _(k):
                c_copy(k).start()

        @pl.when(c < lag)
        def _():
            pair_sum(chunks - lag + c)

        total = sbuf[par, z, cols].astype(jnp.float32)
        for k in range(1, pairs):
            s_copy(c, k).wait_recv()
            total += rbuf[k, cols].astype(jnp.float32)
        xs[cols] = total
        x_copy(c).start()

    @pl.loop(1, fs)
    def _(k):
        c_copy(k).wait_recv()

    sums = cpbuf[0]
    for j in range(1, fs):
        sums += cpbuf[j]
    cps[...] = sums
    cx_copy().start()

    @pl.loop(0, chunks)
    def _(c):
        rows = rows_of(c)
        x_copy(c).wait_recv()
        total = xs[rows] + xr[rows]
        gd_ref[rows] = total
        square = total * total
        while square.shape[1] % 256 == 0:
            middle = square.shape[1] // 2
            square = square[:, :middle] + square[:, middle:]
        rnbuf[me, 0:1, rows] = jnp.sum(square.T, axis=0, keepdims=True)

    @pl.loop(1, fs)
    def _(k):
        n_copy(k).start()

    cx_copy().wait_recv()
    cp_ref[...] = cps[...] + cpx[...]

    @pl.loop(1, fs)
    def _(k):
        n_copy(k).wait_recv()

    norms = rnbuf[0]
    for j in range(1, fs):
        norms += rnbuf[j]
    rn_ref[...] = norms

    cx_copy().wait_send()
    y_first().wait_send()

    @pl.loop(1, pairs)
    def _(k):
        w_copy(k).wait_send()
        y_copy(k).wait_send()

    @pl.loop(1, fs)
    def _(k):
        f_copy(k).wait_send()
        c_copy(k).wait_send()
        n_copy(k).wait_send()

    @pl.loop(0, chunks)
    def _(c):
        x_copy(c).wait_send()
        p_copy(c).wait_send()

        @pl.loop(1, pairs)
        def _(k):
            s_copy(c, k).wait_send()


def out_kernel(gg, gl, cp, gd, rn, ogg, ogl, otg, otl, obg, obl, ogd, orn, sem):
    copies = [
        pltpu.make_async_copy(source, target, sem.at[i])
        for i, (source, target) in enumerate(((gg, ogg), (gl, ogl), (gd, ogd)))
    ]
    for copy in copies:
        copy.start()
    otg[...] = cp[0:3]
    otl[...] = cp[3:6]
    obg[...] = cp[6:7]
    obl[...] = cp[7:8]
    width = rn.shape[1]
    for i in range(rn.shape[0]):
        orn[0:1, i * width:(i + 1) * width] = rn[i:i + 1]
    for copy in copies:
        copy.wait()


def put_out(gg, gl, cp, gd, rn):
    ff = gg.shape[1]
    f32 = jnp.float32
    vmem = pl.BlockSpec(memory_space=pltpu.VMEM)
    hbm = pl.BlockSpec(memory_space=pl.ANY)
    row = jax.ShapeDtypeStruct((1, ff), f32)
    taps = jax.ShapeDtypeStruct((3, ff), f32)
    ogg, ogl, otg, otl, obg, obl, ogd, orn = pl.pallas_call(
        out_kernel,
        out_shape=(
            jax.ShapeDtypeStruct(gg.shape, gg.dtype), jax.ShapeDtypeStruct(gl.shape, gl.dtype),
            taps, taps, row, row, jax.ShapeDtypeStruct(gd.shape, gd.dtype), row),
        in_specs=[vmem] * 5,
        out_specs=(hbm, hbm, vmem, vmem, vmem, vmem, hbm, vmem),
        scratch_shapes=[pltpu.SemaphoreType.DMA((3,))],
        compiler_params=pltpu.CompilerParams(vmem_limit_bytes=2 << 20),
    )(*[pltpu.with_memory_space_constraint(value, pltpu.VMEM) for value in (gg, gl, cp, gd, rn)])
    return ogg, ogl, otg, otl, obg[0], obl[0], ogd, orn[0]


def direct_local(
    fs, pre_gate, pre_linear, taps_gate, taps_linear, bias_gate, bias_linear, down_weight, out_grad
):
    tokens, ff = pre_gate.shape
    dc = down_weight.shape[1]
    chunk = 256
    chunks = ff // chunk
    pairs = fs // 2
    f32, bf16 = jnp.float32, jnp.bfloat16
    vmem = pl.BlockSpec(memory_space=pltpu.VMEM)
    dma = pltpu.SemaphoreType.DMA
    gg, gl, cp, gd, rn = pl.pallas_call(
        functools.partial(kernel, fs, chunk),
        out_shape=(
            pltpu.VMEM((tokens, ff), bf16),
            pltpu.VMEM((tokens, ff), bf16),
            pltpu.VMEM((8, ff), f32),
            pltpu.VMEM((ff, dc), f32),
            pltpu.VMEM((1, ff), f32),
        ),
        in_specs=[vmem] * 8,
        out_specs=(vmem,) * 5,
        scratch_shapes=[
            pltpu.VMEM((fs, ff, dc), bf16),
            pltpu.VMEM((2, pairs, ff, dc), bf16),
            pltpu.VMEM((pairs, ff, dc), bf16),
            pltpu.VMEM((pairs, ff, dc), bf16),
            pltpu.VMEM((ff, dc), f32),
            pltpu.VMEM((ff, dc), f32),
            pltpu.VMEM((fs, 8, ff), f32),
            pltpu.VMEM((8, ff), f32),
            pltpu.VMEM((8, ff), f32),
            pltpu.VMEM((fs, 1, ff), f32),
            dma((pairs,)), dma((pairs,)), dma((pairs,)), dma((pairs,)),
            dma((chunks,)), dma((chunks,)), dma((fs,)), dma((fs,)),
            dma((chunks, pairs)), dma((chunks, pairs)), dma((chunks,)), dma((chunks,)),
            dma((fs,)), dma((fs,)), dma, dma, dma((fs,)), dma((fs,)),
        ],
        compiler_params=pltpu.CompilerParams(
            collective_id=0, has_side_effects=True, vmem_limit_bytes=52 << 20),
    )(pre_gate, pre_linear, taps_gate, taps_linear, bias_gate[None], bias_linear[None],
      down_weight, out_grad)
    return put_out(gg, gl, cp, gd, rn)


def line_kernel(
    fs, unit,
    pg_hbm, pl_hbm, tg_ref, tl_ref, bg_ref, bl_ref, w_hbm, og_hbm,
    gg_ref, gl_ref, cp_ref, gd_ref, rn_ref,
    og, pg, pln, wbuf, xs, xr, own, zb, ys, yr, cpl, cpr, cps, rnb,
    in_sem, og_sem, w_sem, x_send, x_recv, wz_send, wz_recv, wy_send, wy_recv,
    z_send, z_recv, y_send, y_recv, a_send, a_recv,
    c_send, c_recv, b_send, b_recv, n_send, n_recv,
):
    me = lax.axis_index("fs")
    rep = lax.axis_index("rep")
    partner = 1 - rep
    nz = fs // 2
    peers = 2 * fs
    z = me // 2
    y = me % 2
    mate = me + 1 - 2 * y
    flat = rep * fs + me
    tokens, ff = pg_hbm.shape
    dc = w_hbm.shape[1]
    units = ff // unit
    half = unit // 2
    chunks = 2 * units
    ch = half // 2
    span = ff // peers
    wch = unit // 2

    def unit_cols(u):
        return pl.ds(pl.multiple_of(u * unit, unit), unit)

    def half_cols(u, side):
        return pl.ds(pl.multiple_of(u * unit + side * half, half), half)

    def chunk_rows(c, side):
        start = (c // 2) * unit + side * half + (c % 2) * ch
        return pl.ds(pl.multiple_of(start, ch), ch)

    def w_rows(k):
        return pl.ds(pl.multiple_of(k * wch, wch), wch)

    def peer(k):
        at = lax.rem(flat + k, peers)
        return {"rep": at // fs, "fs": at % fs}

    def remote(source, target, send, recv, device):
        return pltpu.make_async_remote_copy(
            src_ref=source, dst_ref=target, send_sem=send, recv_sem=recv,
            device_id=device, device_id_type=MESH)

    def in_copies(u):
        cols = unit_cols(u)
        return (
            pltpu.make_async_copy(pg_hbm.at[:, cols], pg.at[:, cols], in_sem.at[0, u]),
            pltpu.make_async_copy(pl_hbm.at[:, cols], pln.at[:, cols], in_sem.at[1, u]))

    def og_copy():
        return pltpu.make_async_copy(og_hbm, og, og_sem)

    def w_copy():
        return pltpu.make_async_copy(w_hbm, wbuf.at[me], w_sem)

    def x_copy(c):
        return remote(xs.at[c], xr.at[c], x_send, x_recv.at[c], {"rep": partner})

    def wz_copy(way, k, src):
        block = wbuf.at[src * 2 + y, w_rows(k)]
        to = z + 1 if way == 0 else z - 1
        return remote(block, block, wz_send, wz_recv.at[k, src], {"fs": to * 2 + y})

    def wy_copy(k, src):
        block = wbuf.at[src * 2 + y, w_rows(k)]
        return remote(block, block, wy_send, wy_recv.at[k // 2], {"fs": mate})

    def z_up(c, i):
        return remote(
            zb.at[c, i], zb.at[c, i], z_send, z_recv.at[c, i], {"fs": (z + 1) * 2 + y})

    def z_down(c, i):
        slot = jnp.where(i == z - 1, nz, i)
        return remote(
            zb.at[c, i], zb.at[c, slot], z_send, z_recv.at[c, slot], {"fs": (z - 1) * 2 + y})

    def z_arrived(c, slot):
        block = zb.at[c, slot]
        remote(block, block, z_send, z_recv.at[c, slot], {"fs": mate}).wait_recv()

    def all_sent(block, send):
        remote(block, block, send, x_recv.at[0], {"fs": mate}).wait_send()

    def all_arrived(block, recv):
        remote(block, block, x_send, recv, {"fs": mate}).wait_recv()

    def y_copy(c):
        return remote(ys.at[c], yr.at[c], y_send, y_recv.at[c], {"fs": mate})

    def a_copy(c):
        rows = chunk_rows(c, rep)
        return remote(gd_ref.at[rows], gd_ref.at[rows], a_send, a_recv, {"rep": partner})

    def c_copy(k):
        at = lax.rem(flat + k, peers)
        cols = pl.ds(pl.multiple_of(at * span, span), span)
        return remote(cpl.at[:, cols], cpr.at[flat], c_send, c_recv, peer(k))

    def my_span():
        return pl.ds(pl.multiple_of(flat * span, span), span)

    def b_copy(k):
        return remote(cps, cp_ref.at[:, my_span()], b_send, b_recv, peer(k))

    def n_copy(k):
        return remote(rnb.at[flat], rnb.at[flat], n_send, n_recv, peer(k))

    barrier = pltpu.get_barrier_semaphore()

    @pl.loop(1, peers)
    def _(k):
        pl.semaphore_signal(barrier, inc=1, device_id=peer(k), device_id_type=MESH)

    w_copy().start()
    for copy in in_copies(0):
        copy.start()
    og_copy().start()

    @pl.loop(1, units)
    def _(u):
        for copy in in_copies(u):
            copy.start()

    def hidden_half(cols):
        gate_pre = conv_chunk(pg[:, cols].astype(jnp.float32), tg_ref[:, cols], bg_ref[:, cols])
        linear_pre = conv_chunk(pln[:, cols].astype(jnp.float32), tl_ref[:, cols], bl_ref[:, cols])
        return (gate_pre * jax.nn.sigmoid(gate_pre) * linear_pre).astype(jnp.bfloat16)

    def forward(u):
        for copy in in_copies(u):
            copy.wait()
        hidden = jnp.concatenate(
            [hidden_half(half_cols(u, rep)), hidden_half(half_cols(u, partner))], axis=1)
        for j in range(fs):
            part = lax.dot_general(
                hidden, og[:, j * dc:(j + 1) * dc], (((0,), (0,)), ((), ())),
                preferred_element_type=jnp.float32)
            for h in range(2):
                own[2 * u + h, j // 2, j % 2] = part[h * ch:(h + 1) * ch]
                xs[2 * u + h, j // 2, j % 2] = part[half + h * ch:half + (h + 1) * ch].astype(jnp.bfloat16)
    def backward(u):
        cols = unit_cols(u)
        all_arrived(wbuf.at[pl.ds(0, nz), cols], wy_recv.at[u])
        gate_in = pg[:, cols].astype(jnp.float32)
        linear_in = pln[:, cols].astype(jnp.float32)
        taps_gate, taps_linear = tg_ref[:, cols], tl_ref[:, cols]
        gate_pre = conv_chunk(gate_in, taps_gate, bg_ref[:, cols])
        linear_pre = conv_chunk(linear_in, taps_linear, bl_ref[:, cols])
        sigma = jax.nn.sigmoid(gate_pre)
        grad_hidden = jnp.zeros((tokens, unit), jnp.float32)
        for j in range(fs):
            grad_hidden += lax.dot_general(
                og[:, j * dc:(j + 1) * dc], wbuf[j, cols], (((1,), (1,)), ((), ())),
                preferred_element_type=jnp.float32)
        grad_gate_pre = grad_hidden * linear_pre * sigma * (1.0 + gate_pre * (1.0 - sigma))
        grad_linear_pre = grad_hidden * (gate_pre * sigma)
        gg_ref[:, cols] = conv_back_chunk(grad_gate_pre, taps_gate).astype(jnp.bfloat16)
        gl_ref[:, cols] = conv_back_chunk(grad_linear_pre, taps_linear).astype(jnp.bfloat16)
        for j in range(3):
            cpl[j:j + 1, cols] = jnp.sum(
                grad_gate_pre * shift_down(gate_in, 2 - j), axis=0, keepdims=True)
            cpl[j + 3:j + 4, cols] = jnp.sum(
                grad_linear_pre * shift_down(linear_in, 2 - j), axis=0, keepdims=True)
        cpl[6:7, cols] = jnp.sum(grad_gate_pre, axis=0, keepdims=True)
        cpl[7:8, cols] = jnp.sum(grad_linear_pre, axis=0, keepdims=True)
        count = unit // span
        for b in range(count):
            k = lax.rem(u * count + b - flat + peers, peers)

            @pl.when(k != 0)
            def _():
                c_copy(k).start()

    def weights(t):
        @pl.when(t < chunks)
        def _():
            @pl.when(z < nz - 1)
            def _():
                wz_copy(0, t, z).start()

            @pl.when(z > 0)
            def _():
                wz_copy(1, t, z).start()

            wy_copy(t, z).start()

        for d in range(1, nz):
            k = t - d
            live = (k >= 0) & (k < chunks)

            @pl.when(live & (z >= d))
            def _():
                wz_copy(0, k, z - d).wait_recv()

                @pl.when(z < nz - 1)
                def _():
                    wz_copy(0, k, z - d).start()

                wy_copy(k, z - d).start()

            @pl.when(live & (z + d < nz))
            def _():
                wz_copy(1, k, z + d).wait_recv()

                @pl.when(z > 0)
                def _():
                    wz_copy(1, k, z + d).start()

                wy_copy(k, z + d).start()

    def add_step(c, s):
        up = z + nz - s
        down = z - nz + s

        @pl.when(z <= s - 1)
        def _():
            total = own[c, up] + xr[c, up].astype(jnp.float32)

            @pl.when(z > 0)
            def _():
                z_arrived(c, up)
                zb[c, up] = (total + zb[c, up].astype(jnp.float32)).astype(jnp.bfloat16)

            @pl.when(z == 0)
            def _():
                zb[c, up] = total.astype(jnp.bfloat16)

            z_up(c, up).start()

        @pl.when(z >= nz - s)
        def _():
            total = own[c, down] + xr[c, down].astype(jnp.float32)

            @pl.when(z < nz - 1)
            def _():
                z_arrived(c, down)
                zb[c, down] = (total + zb[c, down].astype(jnp.float32)).astype(jnp.bfloat16)

            @pl.when(z == nz - 1)
            def _():
                zb[c, down] = total.astype(jnp.bfloat16)

            z_down(c, down).start()

    def line_end(c):
        own[c, z] += xr[c, z].astype(jnp.float32)

        @pl.when(z > 0)
        def _():
            z_arrived(c, z)
            own[c, z] += zb[c, z].astype(jnp.float32)

        @pl.when(z < nz - 1)
        def _():
            z_arrived(c, nz)
            own[c, z] += zb[c, nz].astype(jnp.float32)

        ys[c] = own[c, z, 1 - y].astype(jnp.bfloat16)
        y_copy(c).start()

    def finish(c):
        y_copy(c).wait_recv()
        gd_ref[chunk_rows(c, rep)] = own[c, z, y] + yr[c].astype(jnp.float32)
        a_copy(c).start()

        @pl.when(c % 2 == 1)
        def _():
            u = c // 2
            total = gd_ref[half_cols(u, rep)]
            square = total * total
            while square.shape[1] % 256 == 0:
                middle = square.shape[1] // 2
                square = square[:, :middle] + square[:, middle:]
            rnb[flat, pl.ds(u, 1)] = jnp.sum(square.T, axis=0, keepdims=True)

    lag = 2
    back_lag = 5
    ticks = chunks + lag + nz

    def send_half(u):
        x_copy(2 * u).start()
        x_copy(2 * u + 1).start()

    def reduce_params():
        cpr[flat] = cpl[:, my_span()]

        all_arrived(cpr.at[pl.ds(0, peers - 1)], c_recv)
        sums = cpr[0]
        for j in range(1, peers):
            sums += cpr[j]
        cps[...] = sums
        cp_ref[:, my_span()] = sums

        @pl.loop(1, peers)
        def _(k):
            b_copy(k).start()

    og_copy().wait()
    forward(0)
    w_copy().wait()
    pl.semaphore_wait(barrier, peers - 1)
    send_half(0)

    @pl.loop(0, ticks)
    def _(t):
        weights(t)

        c = t - lag - nz

        @pl.when((c >= 0) & (c < chunks))
        def _():
            finish(c)

        c = t - lag - nz + 1

        @pl.when((c >= 0) & (c < chunks))
        def _():
            line_end(c)

        for s in range(nz - 1, 0, -1):
            c = t - lag - s + 1

            @pl.when((c >= 0) & (c < chunks))
            def _():
                if s == 1:
                    x_copy(c).wait_recv()
                add_step(c, s)

        @pl.when(t < units - 1)
        def _():
            forward(t + 1)
            send_half(t + 1)

        late = t - back_lag

        @pl.when((late >= 0) & (late % 2 == 0) & (late < chunks))
        def _():
            backward(late // 2)

        @pl.when(t == ticks - 1)
        def _():
            reduce_params()

    @pl.loop(1, peers)
    def _(k):
        n_copy(k).start()

    all_sent(xs, x_send)
    all_sent(ys, y_send)
    all_sent(zb.at[:, pl.ds(0, nz - 1)], z_send)
    all_sent(wbuf.at[pl.ds(0, nz)], wy_send)

    @pl.when((z == 0) | (z == nz - 1))
    def _():
        all_sent(wbuf.at[0], wz_send)

    @pl.when((z > 0) & (z < nz - 1))
    def _():
        all_sent(wbuf.at[pl.ds(0, nz + 1)], wz_send)

    all_sent(cpr.at[pl.ds(0, peers - 1)], c_send)
    all_arrived(rnb.at[pl.ds(0, peers - 1)], n_recv)

    for side in range(2):
        norms = rnb[side * fs]
        for j in range(1, fs):
            norms += rnb[side * fs + j]
        rn_ref[:, side * half:(side + 1) * half] = norms

    all_arrived(cpr.at[pl.ds(0, peers - 1)], b_recv)
    all_arrived(gd_ref.at[pl.ds(0, ff // 2)], a_recv)
    all_sent(gd_ref.at[pl.ds(0, ff // 2)], a_send)
    all_sent(cpr.at[pl.ds(0, peers - 1)], b_send)
    all_sent(rnb.at[pl.ds(0, peers - 1)], n_send)


def line_local(
    fs, pre_gate, pre_linear, taps_gate, taps_linear, bias_gate, bias_linear, down_weight, out_grad
):
    tokens, ff = pre_gate.shape
    dc = down_weight.shape[1]
    unit = 256
    units = ff // unit
    chunks = 2 * units
    ch = unit // 4
    nz = fs // 2
    peers = 2 * fs
    f32, bf16 = jnp.float32, jnp.bfloat16
    vmem = pl.BlockSpec(memory_space=pltpu.VMEM)
    hbm = pl.BlockSpec(memory_space=pl.ANY)
    dma = pltpu.SemaphoreType.DMA
    gg, gl, cp, gd, rn = pl.pallas_call(
        functools.partial(line_kernel, fs, unit),
        out_shape=(
            pltpu.VMEM((tokens, ff), bf16),
            pltpu.VMEM((tokens, ff), bf16),
            pltpu.VMEM((8, ff), f32),
            pltpu.VMEM((ff, dc), f32),
            pltpu.VMEM((units, unit), f32),
        ),
        in_specs=[hbm, hbm, vmem, vmem, vmem, vmem, hbm, hbm],
        out_specs=(vmem,) * 5,
        scratch_shapes=[
            pltpu.VMEM((tokens, out_grad.shape[1]), bf16),
            pltpu.VMEM((tokens, ff), bf16),
            pltpu.VMEM((tokens, ff), bf16),
            pltpu.VMEM((fs, ff, dc), bf16),
            pltpu.VMEM((chunks, nz, 2, ch, dc), bf16),
            pltpu.VMEM((chunks, nz, 2, ch, dc), bf16),
            pltpu.VMEM((chunks, nz, 2, ch, dc), f32),
            pltpu.VMEM((chunks, nz + 1, 2, ch, dc), bf16),
            pltpu.VMEM((chunks, ch, dc), bf16),
            pltpu.VMEM((chunks, ch, dc), bf16),
            pltpu.VMEM((8, ff), f32),
            pltpu.VMEM((peers, 8, ff // peers), f32),
            pltpu.VMEM((8, ff // peers), f32),
            pltpu.VMEM((peers, units, unit // 2), f32),
            dma((2, units)), dma, dma,
            dma, dma((chunks,)), dma, dma((chunks, nz)), dma, dma((units,)),
            dma, dma((chunks, nz + 1)), dma, dma((chunks,)), dma, dma,
            dma, dma, dma, dma, dma, dma,
        ],
        compiler_params=pltpu.CompilerParams(
            collective_id=0, has_side_effects=True, vmem_limit_bytes=55 << 20),
    )(pre_gate, pre_linear, taps_gate, taps_linear, bias_gate[None], bias_linear[None],
      down_weight, out_grad)
    return put_out(gg, gl, cp, gd, rn)


def on_a_line(fs, ff, dc):
    nz = fs // 2
    return fs % 2 == 0 and 2 <= nz <= 4 and ff % (256 * fs) == 0 and dc % 128 == 0


def local(fs, *args):
    if on_a_line(fs, args[0].shape[1], args[6].shape[1]):
        return line_local(fs, *args)
    return direct_local(fs, *args)


def solution(mesh):
    in_specs = (
        P(("rep", "fs"), "tp"),
        P(("rep", "fs"), "tp"),
        P(None, "tp"),
        P(None, "tp"),
        P("tp"),
        P("tp"),
        P("tp", "fs"),
        P(("rep", "fs"), None),
    )
    out_specs = (
        P(("rep", "fs"), "tp"),
        P(("rep", "fs"), "tp"),
        P(None, "tp"),
        P(None, "tp"),
        P("tp"),
        P("tp"),
        P("tp", "fs"),
        P("tp"),
    )
    return jax.shard_map(
        functools.partial(local, mesh.shape["fs"]), mesh=mesh, in_specs=in_specs, out_specs=out_specs, check_vma=False)
```

```python
import functools

import jax
import jax.numpy as jnp
from jax import lax
from jax.experimental import pallas as pl
from jax.experimental.pallas import tpu as pltpu
from jax.sharding import PartitionSpec as P

MESH = pl.DeviceIdType.MESH


def shift_down(values, steps):
    if steps == 0:
        return values
    rows = lax.broadcasted_iota(jnp.int32, values.shape, 0)
    return jnp.where(rows < steps, 0.0, pltpu.roll(values, steps, 0))


def shift_up(values, steps):
    length = values.shape[0]
    rows = lax.broadcasted_iota(jnp.int32, values.shape, 0)
    return jnp.where(rows >= length - steps, 0.0, pltpu.roll(values, length - steps, 0))


def conv_chunk(values, taps, bias):
    return (
        taps[0:1] * shift_down(values, 2)
        + taps[1:2] * shift_down(values, 1)
        + taps[2:3] * values
        + bias
    )


def conv_back_chunk(grads, taps):
    return taps[0:1] * shift_up(grads, 2) + taps[1:2] * shift_up(grads, 1) + taps[2:3] * grads


def kernel(
    fs, chunk,
    pg_ref, pl_ref, tg_ref, tl_ref, bg_ref, bl_ref, w_ref, og_ref,
    gg_ref, gl_ref, cp_ref, gd_ref, rn_ref,
    wbuf, sbuf, pbuf, rbuf, xs, xr, cpbuf, cps, cpx, rnbuf,
    w_send, w_recv, y_send, y_recv, p_send, p_recv, f_send, f_recv, s_send, s_recv, x_send, x_recv,
    c_send, c_recv, cx_send, cx_recv, n_send, n_recv,
):
    me = lax.axis_index("fs")
    rep = lax.axis_index("rep")
    partner = 1 - rep
    pairs = fs // 2
    z = me // 2
    par = me % 2
    mate = me + 1 - 2 * par
    tokens, ff = pg_ref.shape
    dc = w_ref.shape[1]
    chunks = ff // chunk
    half = ff // 2
    lag = chunks // 2
    per = -(-(fs - 1) // chunks)

    def to(k):
        return lax.rem(me + k, fs)

    def rows_of(c):
        return pl.ds(pl.multiple_of(c * chunk, chunk), chunk)

    def shard(z_at, parity):
        return z_at * 2 + parity

    def z_to(k):
        return lax.rem(z + k, pairs)

    def z_from(k):
        return lax.rem(z + pairs - k, pairs)

    def my_half():
        return pl.ds(pl.multiple_of(rep * half, half), half)

    def w_copy(k):
        return pltpu.make_async_remote_copy(
            src_ref=w_ref.at[my_half()], dst_ref=wbuf.at[me, my_half()],
            send_sem=w_send.at[k], recv_sem=w_recv.at[k],
            device_id={"fs": shard(z_to(k), par)}, device_id_type=MESH)

    def y_first():
        return pltpu.make_async_remote_copy(
            src_ref=w_ref.at[my_half()], dst_ref=wbuf.at[me, my_half()],
            send_sem=y_send.at[0], recv_sem=y_recv.at[0],
            device_id={"fs": mate}, device_id_type=MESH)

    def y_copy(k):
        block = wbuf.at[shard(z_from(k), par), my_half()]
        return pltpu.make_async_remote_copy(
            src_ref=block, dst_ref=block,
            send_sem=y_send.at[k], recv_sem=y_recv.at[k],
            device_id={"fs": mate}, device_id_type=MESH)

    def f_copy(item):
        block = wbuf.at[shard(z_from(item % pairs), (par + item // pairs) % 2), my_half()]
        return pltpu.make_async_remote_copy(
            src_ref=block, dst_ref=block,
            send_sem=f_send.at[item], recv_sem=f_recv.at[item],
            device_id={"rep": partner}, device_id_type=MESH)

    def p_copy(c):
        return pltpu.make_async_remote_copy(
            src_ref=sbuf.at[1 - par, :, rows_of(c)], dst_ref=pbuf.at[:, rows_of(c)],
            send_sem=p_send.at[c], recv_sem=p_recv.at[c],
            device_id={"fs": mate}, device_id_type=MESH)

    def s_copy(c, k):
        return pltpu.make_async_remote_copy(
            src_ref=sbuf.at[par, z_to(k), rows_of(c)], dst_ref=rbuf.at[k, rows_of(c)],
            send_sem=s_send.at[c, k], recv_sem=s_recv.at[c, k],
            device_id={"fs": shard(z_to(k), par)}, device_id_type=MESH)

    def pair_sum(c):
        p_copy(c).wait_recv()
        for at in range(pairs):
            both = sbuf[par, at, rows_of(c)].astype(jnp.float32) + pbuf[at, rows_of(c)].astype(jnp.float32)
            sbuf[par, at, rows_of(c)] = both.astype(jnp.bfloat16)

        @pl.loop(1, pairs)
        def _(k):
            s_copy(c, k).start()

    def x_copy(c):
        return pltpu.make_async_remote_copy(
            src_ref=xs.at[rows_of(c)], dst_ref=xr.at[rows_of(c)],
            send_sem=x_send.at[c], recv_sem=x_recv.at[c],
            device_id={"rep": partner}, device_id_type=MESH)

    def c_copy(k):
        return pltpu.make_async_remote_copy(
            src_ref=cpbuf.at[me], dst_ref=cpbuf.at[me],
            send_sem=c_send.at[k], recv_sem=c_recv.at[k],
            device_id={"fs": to(k)}, device_id_type=MESH)

    def cx_copy():
        return pltpu.make_async_remote_copy(
            src_ref=cps, dst_ref=cpx, send_sem=cx_send, recv_sem=cx_recv,
            device_id={"rep": partner}, device_id_type=MESH)

    def n_copy(k):
        return pltpu.make_async_remote_copy(
            src_ref=rnbuf.at[me], dst_ref=rnbuf.at[me],
            send_sem=n_send.at[k], recv_sem=n_recv.at[k],
            device_id={"fs": to(k)}, device_id_type=MESH)

    barrier = pltpu.get_barrier_semaphore()

    @pl.loop(1, fs)
    def _(k):
        pl.semaphore_signal(barrier, inc=1, device_id={"fs": to(k)}, device_id_type=MESH)

    pl.semaphore_signal(barrier, inc=1, device_id={"rep": partner}, device_id_type=MESH)
    pl.semaphore_wait(barrier, fs)

    y_first().start()

    @pl.loop(1, pairs)
    def _(k):
        w_copy(k).start()

    wbuf[me] = w_ref[...]

    @pl.loop(0, chunks)
    def _(c):
        cols = rows_of(c)
        gate_pre = conv_chunk(
            pg_ref[:, cols].astype(jnp.float32), tg_ref[:, cols], bg_ref[:, cols])
        linear_pre = conv_chunk(
            pl_ref[:, cols].astype(jnp.float32), tl_ref[:, cols], bl_ref[:, cols])
        hidden = (gate_pre * jax.nn.sigmoid(gate_pre) * linear_pre).astype(jnp.bfloat16)
        for j in range(fs):
            part = lax.dot_general(
                hidden, og_ref[:, j * dc:(j + 1) * dc], (((0,), (0,)), ((), ())),
                preferred_element_type=jnp.float32)
            sbuf[j % 2, j // 2, cols] = part.astype(jnp.bfloat16)

        p_copy(c).start()

        @pl.when(c >= lag)
        def _():
            pair_sum(c - lag)

        for step in range(per):
            k = c * per + step + 1

            @pl.when(k < pairs)
            def _():
                w_copy(k).wait_recv()
                y_copy(k).start()
                f_copy(k).start()

            @pl.when((k >= pairs) & (k < fs))
            def _():
                y_copy(k - pairs).wait_recv()
                f_copy(k).start()

    @pl.loop(1, fs)
    def _(k):
        f_copy(k).wait_recv()

    @pl.loop(0, chunks)
    def _(c):
        cols = rows_of(c)
        gate_in = pg_ref[:, cols].astype(jnp.float32)
        linear_in = pl_ref[:, cols].astype(jnp.float32)
        taps_gate, taps_linear = tg_ref[:, cols], tl_ref[:, cols]
        gate_pre = conv_chunk(gate_in, taps_gate, bg_ref[:, cols])
        linear_pre = conv_chunk(linear_in, taps_linear, bl_ref[:, cols])
        sigma = jax.nn.sigmoid(gate_pre)
        grad_hidden = jnp.zeros((tokens, chunk), jnp.float32)
        for j in range(fs):
            grad_hidden += lax.dot_general(
                og_ref[:, j * dc:(j + 1) * dc], wbuf[j, cols], (((1,), (1,)), ((), ())),
                preferred_element_type=jnp.float32)
        grad_gate_pre = grad_hidden * linear_pre * sigma * (1.0 + gate_pre * (1.0 - sigma))
        grad_linear_pre = grad_hidden * (gate_pre * sigma)
        gg_ref[:, cols] = conv_back_chunk(grad_gate_pre, taps_gate).astype(jnp.bfloat16)
        gl_ref[:, cols] = conv_back_chunk(grad_linear_pre, taps_linear).astype(jnp.bfloat16)
        for j in range(3):
            cpbuf[me, j:j + 1, cols] = jnp.sum(
                grad_gate_pre * shift_down(gate_in, 2 - j), axis=0, keepdims=True)
            cpbuf[me, j + 3:j + 4, cols] = jnp.sum(
                grad_linear_pre * shift_down(linear_in, 2 - j), axis=0, keepdims=True)
        cpbuf[me, 6:7, cols] = jnp.sum(grad_gate_pre, axis=0, keepdims=True)
        cpbuf[me, 7:8, cols] = jnp.sum(grad_linear_pre, axis=0, keepdims=True)

        @pl.when(c == chunks - 1)
        def _():
            @pl.loop(1, fs)
            def _(k):
                c_copy(k).start()

        @pl.when(c < lag)
        def _():
            pair_sum(chunks - lag + c)

        total = sbuf[par, z, cols].astype(jnp.float32)
        for k in range(1, pairs):
            s_copy(c, k).wait_recv()
            total += rbuf[k, cols].astype(jnp.float32)
        xs[cols] = total
        x_copy(c).start()

    @pl.loop(1, fs)
    def _(k):
        c_copy(k).wait_recv()

    sums = cpbuf[0]
    for j in range(1, fs):
        sums += cpbuf[j]
    cps[...] = sums
    cx_copy().start()

    @pl.loop(0, chunks)
    def _(c):
        rows = rows_of(c)
        x_copy(c).wait_recv()
        total = xs[rows] + xr[rows]
        gd_ref[rows] = total
        square = total * total
        while square.shape[1] % 256 == 0:
            middle = square.shape[1] // 2
            square = square[:, :middle] + square[:, middle:]
        rnbuf[me, 0:1, rows] = jnp.sum(square.T, axis=0, keepdims=True)

    @pl.loop(1, fs)
    def _(k):
        n_copy(k).start()

    cx_copy().wait_recv()
    cp_ref[...] = cps[...] + cpx[...]

    @pl.loop(1, fs)
    def _(k):
        n_copy(k).wait_recv()

    norms = rnbuf[0]
    for j in range(1, fs):
        norms += rnbuf[j]
    rn_ref[...] = norms

    cx_copy().wait_send()
    y_first().wait_send()

    @pl.loop(1, pairs)
    def _(k):
        w_copy(k).wait_send()
        y_copy(k).wait_send()

    @pl.loop(1, fs)
    def _(k):
        f_copy(k).wait_send()
        c_copy(k).wait_send()
        n_copy(k).wait_send()

    @pl.loop(0, chunks)
    def _(c):
        x_copy(c).wait_send()
        p_copy(c).wait_send()

        @pl.loop(1, pairs)
        def _(k):
            s_copy(c, k).wait_send()


def out_kernel(gg, gl, cp, gd, rn, ogg, ogl, otg, otl, obg, obl, ogd, orn, sem):
    copies = [
        pltpu.make_async_copy(source, target, sem.at[i])
        for i, (source, target) in enumerate(((gg, ogg), (gl, ogl), (gd, ogd)))
    ]
    for copy in copies:
        copy.start()
    otg[...] = cp[0:3]
    otl[...] = cp[3:6]
    obg[...] = cp[6:7]
    obl[...] = cp[7:8]
    width = rn.shape[1]
    for i in range(rn.shape[0]):
        orn[0:1, i * width:(i + 1) * width] = rn[i:i + 1]
    for copy in copies:
        copy.wait()


def put_out(gg, gl, cp, gd, rn):
    ff = gg.shape[1]
    f32 = jnp.float32
    vmem = pl.BlockSpec(memory_space=pltpu.VMEM)
    hbm = pl.BlockSpec(memory_space=pl.ANY)
    row = jax.ShapeDtypeStruct((1, ff), f32)
    taps = jax.ShapeDtypeStruct((3, ff), f32)
    ogg, ogl, otg, otl, obg, obl, ogd, orn = pl.pallas_call(
        out_kernel,
        out_shape=(
            jax.ShapeDtypeStruct(gg.shape, gg.dtype), jax.ShapeDtypeStruct(gl.shape, gl.dtype),
            taps, taps, row, row, jax.ShapeDtypeStruct(gd.shape, gd.dtype), row),
        in_specs=[vmem] * 5,
        out_specs=(hbm, hbm, vmem, vmem, vmem, vmem, hbm, vmem),
        scratch_shapes=[pltpu.SemaphoreType.DMA((3,))],
        compiler_params=pltpu.CompilerParams(vmem_limit_bytes=2 << 20),
    )(*[pltpu.with_memory_space_constraint(value, pltpu.VMEM) for value in (gg, gl, cp, gd, rn)])
    return ogg, ogl, otg, otl, obg[0], obl[0], ogd, orn[0]


def direct_local(
    fs, pre_gate, pre_linear, taps_gate, taps_linear, bias_gate, bias_linear, down_weight, out_grad
):
    tokens, ff = pre_gate.shape
    dc = down_weight.shape[1]
    chunk = 256
    chunks = ff // chunk
    pairs = fs // 2
    f32, bf16 = jnp.float32, jnp.bfloat16
    vmem = pl.BlockSpec(memory_space=pltpu.VMEM)
    dma = pltpu.SemaphoreType.DMA
    gg, gl, cp, gd, rn = pl.pallas_call(
        functools.partial(kernel, fs, chunk),
        out_shape=(
            pltpu.VMEM((tokens, ff), bf16),
            pltpu.VMEM((tokens, ff), bf16),
            pltpu.VMEM((8, ff), f32),
            pltpu.VMEM((ff, dc), f32),
            pltpu.VMEM((1, ff), f32),
        ),
        in_specs=[vmem] * 8,
        out_specs=(vmem,) * 5,
        scratch_shapes=[
            pltpu.VMEM((fs, ff, dc), bf16),
            pltpu.VMEM((2, pairs, ff, dc), bf16),
            pltpu.VMEM((pairs, ff, dc), bf16),
            pltpu.VMEM((pairs, ff, dc), bf16),
            pltpu.VMEM((ff, dc), f32),
            pltpu.VMEM((ff, dc), f32),
            pltpu.VMEM((fs, 8, ff), f32),
            pltpu.VMEM((8, ff), f32),
            pltpu.VMEM((8, ff), f32),
            pltpu.VMEM((fs, 1, ff), f32),
            dma((pairs,)), dma((pairs,)), dma((pairs,)), dma((pairs,)),
            dma((chunks,)), dma((chunks,)), dma((fs,)), dma((fs,)),
            dma((chunks, pairs)), dma((chunks, pairs)), dma((chunks,)), dma((chunks,)),
            dma((fs,)), dma((fs,)), dma, dma, dma((fs,)), dma((fs,)),
        ],
        compiler_params=pltpu.CompilerParams(
            collective_id=0, has_side_effects=True, vmem_limit_bytes=52 << 20),
    )(pre_gate, pre_linear, taps_gate, taps_linear, bias_gate[None], bias_linear[None],
      down_weight, out_grad)
    return put_out(gg, gl, cp, gd, rn)


def line_kernel(
    fs, unit,
    pg_hbm, pl_hbm, tg_ref, tl_ref, bg_ref, bl_ref, w_hbm, og_hbm,
    gg_ref, gl_ref, cp_ref, gd_ref, rn_ref,
    og, pg, pln, wbuf, xs, xr, own, zb, ys, yr, fsum, fr, cpl, cpr, nrm, blk, tail,
    in_sem, og_sem, w_sem, x_send, x_recv, wz_send, wz_recv, wy_send, wy_recv,
    z_send, z_recv, y_send, y_recv, a_send, a_recv, f_send, f_recv,
    c_send, c_recv, b_send, b_recv, t_send, t_recv,
):
    me = lax.axis_index("fs")
    rep = lax.axis_index("rep")
    partner = 1 - rep
    nz = fs // 2
    peers = 2 * fs
    z = me // 2
    y = me % 2
    mate = me + 1 - 2 * y
    flat = rep * fs + me
    tokens, ff = pg_hbm.shape
    dc = w_hbm.shape[1]
    units = ff // unit
    half = unit // 2
    chunks = 2 * units
    split = chunks - 2
    spare = chunks + 2
    ch = half // 2
    span = ff // peers
    owners = (units - 1) * unit // span
    wch = unit // 2

    def unit_cols(u):
        return pl.ds(pl.multiple_of(u * unit, unit), unit)

    def half_cols(u, side):
        return pl.ds(pl.multiple_of(u * unit + side * half, half), half)

    def chunk_rows(c, side):
        start = (c // 2) * unit + side * half + (c % 2) * ch
        return pl.ds(pl.multiple_of(start, ch), ch)

    def w_rows(k):
        return pl.ds(pl.multiple_of(k * wch, wch), wch)

    def peer(k):
        at = lax.rem(flat + k, peers)
        return {"rep": at // fs, "fs": at % fs}

    def remote(source, target, send, recv, device):
        return pltpu.make_async_remote_copy(
            src_ref=source, dst_ref=target, send_sem=send, recv_sem=recv,
            device_id=device, device_id_type=MESH)

    def in_copies(u):
        cols = unit_cols(u)
        return (
            pltpu.make_async_copy(pg_hbm.at[:, cols], pg.at[:, cols], in_sem.at[0, u]),
            pltpu.make_async_copy(pl_hbm.at[:, cols], pln.at[:, cols], in_sem.at[1, u]))

    def og_copy():
        return pltpu.make_async_copy(og_hbm, og, og_sem)

    def w_copy():
        return pltpu.make_async_copy(w_hbm, wbuf.at[me], w_sem)

    def x_copy(c):
        return remote(xs.at[c], xr.at[c], x_send, x_recv.at[c], {"rep": partner})

    def wz_copy(way, k, src):
        block = wbuf.at[src * 2 + y, w_rows(k)]
        to = z + 1 if way == 0 else z - 1
        return remote(block, block, wz_send, wz_recv.at[k, src], {"fs": to * 2 + y})

    def wy_copy(k, src):
        block = wbuf.at[src * 2 + y, w_rows(k)]
        return remote(block, block, wy_send, wy_recv.at[k // 2], {"fs": mate})

    def z_up(c, i):
        return remote(
            zb.at[c, i], zb.at[c, i], z_send, z_recv.at[c, i], {"fs": (z + 1) * 2 + y})

    def z_down(c, i):
        slot = jnp.where(i == z - 1, nz, i)
        return remote(
            zb.at[c, i], zb.at[c, slot], z_send, z_recv.at[c, slot], {"fs": (z - 1) * 2 + y})

    def z_arrived(c, slot):
        block = zb.at[c, slot]
        remote(block, block, z_send, z_recv.at[c, slot], {"fs": mate}).wait_recv()

    def all_sent(block, send):
        remote(block, block, send, x_recv.at[0], {"fs": mate}).wait_send()

    def all_arrived(block, recv):
        remote(block, block, x_send, recv, {"fs": mate}).wait_recv()

    def y_copy(c):
        return remote(ys.at[c], yr.at[c], y_send, y_recv.at[c], {"fs": mate})

    def a_copy(c):
        rows = chunk_rows(c, rep)
        return remote(gd_ref.at[rows], gd_ref.at[rows], a_send, a_recv, {"rep": partner})

    def f_copy(f):
        return remote(fsum.at[f], fr.at[f], f_send, f_recv, {"rep": partner})

    def c_copy(k):
        at = lax.rem(flat + k, peers)
        cols = pl.ds(pl.multiple_of(at * span, span), span)
        return remote(cpl.at[:, cols], cpr.at[flat], c_send, c_recv, peer(k))

    def my_span():
        return pl.ds(pl.multiple_of(flat * span, span), span)

    def b_copy(k):
        return remote(blk.at[flat], blk.at[flat], b_send, b_recv, peer(k))

    def t_copy(k):
        return remote(tail.at[flat], tail.at[flat], t_send, t_recv, peer(k))

    barrier = pltpu.get_barrier_semaphore()

    @pl.loop(1, peers)
    def _(k):
        pl.semaphore_signal(barrier, inc=1, device_id=peer(k), device_id_type=MESH)

    w_copy().start()
    for copy in in_copies(0):
        copy.start()
    og_copy().start()

    @pl.loop(1, units)
    def _(u):
        for copy in in_copies(u):
            copy.start()

    def hidden_half(cols):
        gate_pre = conv_chunk(pg[:, cols].astype(jnp.float32), tg_ref[:, cols], bg_ref[:, cols])
        linear_pre = conv_chunk(pln[:, cols].astype(jnp.float32), tl_ref[:, cols], bl_ref[:, cols])
        return (gate_pre * jax.nn.sigmoid(gate_pre) * linear_pre).astype(jnp.bfloat16)

    def forward(u):
        for copy in in_copies(u):
            copy.wait()
        last = u == units - 1
        mine_at = jnp.where(last, split + 2 * rep, 2 * u)
        theirs_at = jnp.where(last, split + 2 * partner, spare)
        hidden = jnp.concatenate(
            [hidden_half(half_cols(u, rep)), hidden_half(half_cols(u, partner))], axis=1)
        for j in range(fs):
            part = lax.dot_general(
                hidden, og[:, j * dc:(j + 1) * dc], (((0,), (0,)), ((), ())),
                preferred_element_type=jnp.float32)
            for h in range(2):
                theirs = part[half + h * ch:half + (h + 1) * ch]
                own[mine_at + h, j // 2, j % 2] = part[h * ch:(h + 1) * ch]
                own[theirs_at + h, j // 2, j % 2] = theirs
                xs[2 * u + h, j // 2, j % 2] = theirs.astype(jnp.bfloat16)
    def backward(u):
        cols = unit_cols(u)
        all_arrived(wbuf.at[pl.ds(0, nz), cols], wy_recv.at[u])
        gate_in = pg[:, cols].astype(jnp.float32)
        linear_in = pln[:, cols].astype(jnp.float32)
        taps_gate, taps_linear = tg_ref[:, cols], tl_ref[:, cols]
        gate_pre = conv_chunk(gate_in, taps_gate, bg_ref[:, cols])
        linear_pre = conv_chunk(linear_in, taps_linear, bl_ref[:, cols])
        sigma = jax.nn.sigmoid(gate_pre)
        grad_hidden = jnp.zeros((tokens, unit), jnp.float32)
        for j in range(fs):
            grad_hidden += lax.dot_general(
                og[:, j * dc:(j + 1) * dc], wbuf[j, cols], (((1,), (1,)), ((), ())),
                preferred_element_type=jnp.float32)
        grad_gate_pre = grad_hidden * linear_pre * sigma * (1.0 + gate_pre * (1.0 - sigma))
        grad_linear_pre = grad_hidden * (gate_pre * sigma)
        gg_ref[:, cols] = conv_back_chunk(grad_gate_pre, taps_gate).astype(jnp.bfloat16)
        gl_ref[:, cols] = conv_back_chunk(grad_linear_pre, taps_linear).astype(jnp.bfloat16)
        for j in range(3):
            cpl[j:j + 1, cols] = jnp.sum(
                grad_gate_pre * shift_down(gate_in, 2 - j), axis=0, keepdims=True)
            cpl[j + 3:j + 4, cols] = jnp.sum(
                grad_linear_pre * shift_down(linear_in, 2 - j), axis=0, keepdims=True)
        cpl[6:7, cols] = jnp.sum(grad_gate_pre, axis=0, keepdims=True)
        cpl[7:8, cols] = jnp.sum(grad_linear_pre, axis=0, keepdims=True)
        count = unit // span
        for b in range(count):
            k = lax.rem(u * count + b - flat + peers, peers)

            @pl.when((k != 0) & (u < units - 1))
            def _():
                c_copy(k).start()

    def own_z(k):
        @pl.when(z < nz - 1)
        def _():
            wz_copy(0, k, z).start()

        @pl.when(z > 0)
        def _():
            wz_copy(1, k, z).start()

    def weights(t):
        @pl.when(t + ahead_z < chunks)
        def _():
            own_z(t + ahead_z)

        @pl.when(t + ahead_y < chunks)
        def _():
            wy_copy(t + ahead_y, z).start()

        for d in range(1, nz):
            k = t - d + early
            live = (k >= 0) & (k < chunks)

            @pl.when(live & (z >= d))
            def _():
                wz_copy(0, k, z - d).wait_recv()

                @pl.when(z < nz - 1)
                def _():
                    wz_copy(0, k, z - d).start()

                wy_copy(k, z - d).start()

            @pl.when(live & (z + d < nz))
            def _():
                wz_copy(1, k, z + d).wait_recv()

                @pl.when(z > 0)
                def _():
                    wz_copy(1, k, z + d).start()

                wy_copy(k, z + d).start()

    def add_step(c, s):
        up = z + nz - s
        down = z - nz + s

        @pl.when(z <= s - 1)
        def _():
            total = own[c, up]

            @pl.when(z > 0)
            def _():
                z_arrived(c, up)
                zb[c, up] = (total + zb[c, up].astype(jnp.float32)).astype(jnp.bfloat16)

            @pl.when(z == 0)
            def _():
                zb[c, up] = total.astype(jnp.bfloat16)

            z_up(c, up).start()

        @pl.when(z >= nz - s)
        def _():
            total = own[c, down]

            @pl.when(z < nz - 1)
            def _():
                z_arrived(c, down)
                zb[c, down] = (total + zb[c, down].astype(jnp.float32)).astype(jnp.bfloat16)

            @pl.when(z == nz - 1)
            def _():
                zb[c, down] = total.astype(jnp.bfloat16)

            z_down(c, down).start()

    def line_end(c):
        @pl.when(z > 0)
        def _():
            z_arrived(c, z)
            own[c, z] += zb[c, z].astype(jnp.float32)

        @pl.when(z < nz - 1)
        def _():
            z_arrived(c, nz)
            own[c, z] += zb[c, nz].astype(jnp.float32)

        ys[c] = own[c, z, 1 - y].astype(jnp.bfloat16)
        y_copy(c).start()

    def finish(c):
        y_copy(c).wait_recv()
        gd_ref[chunk_rows(c, rep)] = own[c, z, y] + yr[c].astype(jnp.float32)
        a_copy(c).start()

        @pl.when(c % 2 == 1)
        def _():
            norms_of(c // 2)

    def norms_of(u):
        total = gd_ref[half_cols(u, rep)]
        square = total * total
        while square.shape[1] % 256 == 0:
            middle = square.shape[1] // 2
            square = square[:, :middle] + square[:, middle:]
        nrm[pl.ds(u, 1)] = jnp.sum(square.T, axis=0, keepdims=True)

    def finish_both(f):
        c = split + f
        y_copy(c).wait_recv()
        fsum[f] = own[c, z, y] + yr[c].astype(jnp.float32)
        f_copy(f).start()

    def join_both():
        all_arrived(fr, f_recv)
        for f in range(4):
            rows = chunk_rows(split + f % 2, f // 2)
            gd_ref[rows] = fsum[f] + fr[f]
        norms_of(units - 1)

    lag = 2
    back_lag = 5
    ahead_y = 3
    early = 0
    ahead_z = 1
    ticks = max(split + lag + nz, chunks - 1 + back_lag)

    def send_half(u):
        x_copy(2 * u).start()
        x_copy(2 * u + 1).start()

    def reduce_params():
        cpr[flat] = cpl[:, my_span()]

        all_arrived(cpr.at[pl.ds(0, peers - 1)], c_recv)
        sums = cpr[0]
        for j in range(1, peers):
            sums += cpr[j]
        blk[flat] = sums

        @pl.loop(1, peers)
        def _(k):
            b_copy(k).start()

    w_copy().wait()
    tail[flat] = jnp.zeros(tail.shape[1:], jnp.float32)
    pl.semaphore_wait(barrier, peers - 1)
    for k in range(ahead_z):
        own_z(k)
    for k in range(ahead_y):
        wy_copy(k, z).start()
    og_copy().wait()
    forward(0)
    send_half(0)

    @pl.loop(0, ticks)
    def _(t):
        weights(t)

        late = t - back_lag

        @pl.when((late >= 0) & (late % 2 == 0) & (late < chunks))
        def _():
            backward(late // 2)

        c = t - lag - nz

        @pl.when((c >= 0) & (c < split))
        def _():
            finish(c)

        c = t - lag - nz + 1

        @pl.when((c >= 0) & (c < split))
        def _():
            line_end(c)

        for s in range(nz - 1, 0, -1):
            c = t - lag - s + 1

            @pl.when((c >= 0) & (c < split))
            def _():
                if s == 1:
                    x_copy(c).wait_recv()
                    own[c] += xr[c].astype(jnp.float32)
                add_step(c, s)

        @pl.loop(0, 4)
        def _(f):
            s = t - 2 * f

            @pl.when(s == nz + 1)
            def _():
                finish_both(f)

            @pl.when(s == nz)
            def _():
                line_end(split + f)

            @pl.when((s >= 1) & (s < nz))
            def _():
                add_step(split + f, s)

        @pl.when(t < units - 1)
        def _():
            forward(jnp.where(t == 0, units - 1, t))

            @pl.when(t > 0)
            def _():
                send_half(t)

        @pl.when((t == ticks - 2) & (flat < owners))
        def _():
            reduce_params()

    join_both()
    tail[flat, 0:8] = cpl[:, ff - unit:]
    tail[flat, 8:, 0:half] = nrm[...]

    @pl.loop(1, peers)
    def _(k):
        t_copy(k).start()

    all_sent(xs.at[pl.ds(0, split)], x_send)
    all_sent(fsum, f_send)
    all_sent(ys, y_send)
    all_sent(zb.at[:, pl.ds(0, nz - 1)], z_send)
    all_sent(wbuf.at[pl.ds(0, nz)], wy_send)

    @pl.when((z == 0) | (z == nz - 1))
    def _():
        all_sent(wbuf.at[0], wz_send)

    @pl.when((z > 0) & (z < nz - 1))
    def _():
        all_sent(wbuf.at[pl.ds(0, nz + 1)], wz_send)

    @pl.when(flat < owners)
    def _():
        all_sent(cpr.at[pl.ds(0, owners - 1)], c_send)
        all_sent(blk.at[pl.ds(0, peers - 1)], b_send)
        all_arrived(blk.at[pl.ds(0, owners - 1)], b_recv)

    @pl.when(flat >= owners)
    def _():
        all_sent(cpr.at[pl.ds(0, owners)], c_send)
        all_arrived(blk.at[pl.ds(0, owners)], b_recv)

    for q in range(owners):
        cp_ref[:, q * span:(q + 1) * span] = blk[q]
    all_arrived(tail.at[pl.ds(0, peers - 1)], t_recv)
    sums = tail[0, 0:8]
    for q in range(1, peers):
        sums += tail[q, 0:8]
    cp_ref[:, ff - unit:] = sums
    for side in range(2):
        norms = tail[side * fs, 8:, 0:half]
        for j in range(1, fs):
            norms += tail[side * fs + j, 8:, 0:half]
        rn_ref[:, side * half:(side + 1) * half] = norms

    all_arrived(gd_ref.at[pl.ds(0, split * ch)], a_recv)
    all_sent(gd_ref.at[pl.ds(0, split * ch)], a_send)
    all_sent(tail.at[pl.ds(0, peers - 1)], t_send)


def line_local(
    fs, pre_gate, pre_linear, taps_gate, taps_linear, bias_gate, bias_linear, down_weight, out_grad
):
    tokens, ff = pre_gate.shape
    dc = down_weight.shape[1]
    unit = 256
    units = ff // unit
    chunks = 2 * units
    ch = unit // 4
    nz = fs // 2
    peers = 2 * fs
    f32, bf16 = jnp.float32, jnp.bfloat16
    vmem = pl.BlockSpec(memory_space=pltpu.VMEM)
    hbm = pl.BlockSpec(memory_space=pl.ANY)
    dma = pltpu.SemaphoreType.DMA
    gg, gl, cp, gd, rn = pl.pallas_call(
        functools.partial(line_kernel, fs, unit),
        out_shape=(
            pltpu.VMEM((tokens, ff), bf16),
            pltpu.VMEM((tokens, ff), bf16),
            pltpu.VMEM((8, ff), f32),
            pltpu.VMEM((ff, dc), f32),
            pltpu.VMEM((units, unit), f32),
        ),
        in_specs=[hbm, hbm, vmem, vmem, vmem, vmem, hbm, hbm],
        out_specs=(vmem,) * 5,
        scratch_shapes=[
            pltpu.VMEM((tokens, out_grad.shape[1]), bf16),
            pltpu.VMEM((tokens, ff), bf16),
            pltpu.VMEM((tokens, ff), bf16),
            pltpu.VMEM((fs, ff, dc), bf16),
            pltpu.VMEM((chunks, nz, 2, ch, dc), bf16),
            pltpu.VMEM((chunks - 2, nz, 2, ch, dc), bf16),
            pltpu.VMEM((chunks + 4, nz, 2, ch, dc), f32),
            pltpu.VMEM((chunks + 2, nz + 1, 2, ch, dc), bf16),
            pltpu.VMEM((chunks + 2, ch, dc), bf16),
            pltpu.VMEM((chunks + 2, ch, dc), bf16),
            pltpu.VMEM((4, ch, dc), f32),
            pltpu.VMEM((4, ch, dc), f32),
            pltpu.VMEM((8, ff), f32),
            pltpu.VMEM((peers, 8, ff // peers), f32),
            pltpu.VMEM((units, unit // 2), f32),
            pltpu.VMEM((peers, 8, ff // peers), f32),
            pltpu.VMEM((peers, 8 + units, unit), f32),
            dma((2, units)), dma, dma,
            dma, dma((chunks,)), dma, dma((chunks, nz)), dma, dma((units,)),
            dma, dma((chunks + 2, nz + 1)), dma, dma((chunks + 2,)), dma, dma, dma, dma,
            dma, dma, dma, dma, dma, dma,
        ],
        compiler_params=pltpu.CompilerParams(
            collective_id=0, has_side_effects=True, vmem_limit_bytes=55 << 20),
    )(pre_gate, pre_linear, taps_gate, taps_linear, bias_gate[None], bias_linear[None],
      down_weight, out_grad)
    return put_out(gg, gl, cp, gd, rn)


def on_a_line(fs, ff, dc):
    nz = fs // 2
    return fs % 2 == 0 and 2 <= nz <= 4 and ff % (256 * fs) == 0 and dc % 128 == 0


def local(fs, *args):
    if on_a_line(fs, args[0].shape[1], args[6].shape[1]):
        return line_local(fs, *args)
    return direct_local(fs, *args)


def solution(mesh):
    in_specs = (
        P(("rep", "fs"), "tp"),
        P(("rep", "fs"), "tp"),
        P(None, "tp"),
        P(None, "tp"),
        P("tp"),
        P("tp"),
        P("tp", "fs"),
        P(("rep", "fs"), None),
    )
    out_specs = (
        P(("rep", "fs"), "tp"),
        P(("rep", "fs"), "tp"),
        P(None, "tp"),
        P(None, "tp"),
        P("tp"),
        P("tp"),
        P("tp", "fs"),
        P("tp"),
    )
    return jax.shard_map(
        functools.partial(local, mesh.shape["fs"]), mesh=mesh, in_specs=in_specs, out_specs=out_specs, check_vma=False)
```

```python
import functools

import jax
import jax.numpy as jnp
from jax import lax
from jax.experimental import pallas as pl
from jax.experimental.pallas import tpu as pltpu
from jax.sharding import PartitionSpec as P

MESH = pl.DeviceIdType.MESH


def shift_down(values, steps):
    if steps == 0:
        return values
    rows = lax.broadcasted_iota(jnp.int32, values.shape, 0)
    return jnp.where(rows < steps, 0.0, pltpu.roll(values, steps, 0))


def shift_up(values, steps):
    length = values.shape[0]
    rows = lax.broadcasted_iota(jnp.int32, values.shape, 0)
    return jnp.where(rows >= length - steps, 0.0, pltpu.roll(values, length - steps, 0))


def conv_chunk(values, taps, bias):
    return (
        taps[0:1] * shift_down(values, 2)
        + taps[1:2] * shift_down(values, 1)
        + taps[2:3] * values
        + bias
    )


def conv_back_chunk(grads, taps):
    return taps[0:1] * shift_up(grads, 2) + taps[1:2] * shift_up(grads, 1) + taps[2:3] * grads


def kernel(
    fs, chunk,
    pg_ref, pl_ref, tg_ref, tl_ref, bg_ref, bl_ref, w_ref, og_ref,
    gg_ref, gl_ref, cp_ref, gd_ref, rn_ref,
    wbuf, sbuf, pbuf, rbuf, xs, xr, cpbuf, cps, cpx, rnbuf,
    w_send, w_recv, y_send, y_recv, p_send, p_recv, f_send, f_recv, s_send, s_recv, x_send, x_recv,
    c_send, c_recv, cx_send, cx_recv, n_send, n_recv,
):
    me = lax.axis_index("fs")
    rep = lax.axis_index("rep")
    partner = 1 - rep
    pairs = fs // 2
    z = me // 2
    par = me % 2
    mate = me + 1 - 2 * par
    tokens, ff = pg_ref.shape
    dc = w_ref.shape[1]
    chunks = ff // chunk
    half = ff // 2
    lag = chunks // 2
    per = -(-(fs - 1) // chunks)

    def to(k):
        return lax.rem(me + k, fs)

    def rows_of(c):
        return pl.ds(pl.multiple_of(c * chunk, chunk), chunk)

    def shard(z_at, parity):
        return z_at * 2 + parity

    def z_to(k):
        return lax.rem(z + k, pairs)

    def z_from(k):
        return lax.rem(z + pairs - k, pairs)

    def my_half():
        return pl.ds(pl.multiple_of(rep * half, half), half)

    def w_copy(k):
        return pltpu.make_async_remote_copy(
            src_ref=w_ref.at[my_half()], dst_ref=wbuf.at[me, my_half()],
            send_sem=w_send.at[k], recv_sem=w_recv.at[k],
            device_id={"fs": shard(z_to(k), par)}, device_id_type=MESH)

    def y_first():
        return pltpu.make_async_remote_copy(
            src_ref=w_ref.at[my_half()], dst_ref=wbuf.at[me, my_half()],
            send_sem=y_send.at[0], recv_sem=y_recv.at[0],
            device_id={"fs": mate}, device_id_type=MESH)

    def y_copy(k):
        block = wbuf.at[shard(z_from(k), par), my_half()]
        return pltpu.make_async_remote_copy(
            src_ref=block, dst_ref=block,
            send_sem=y_send.at[k], recv_sem=y_recv.at[k],
            device_id={"fs": mate}, device_id_type=MESH)

    def f_copy(item):
        block = wbuf.at[shard(z_from(item % pairs), (par + item // pairs) % 2), my_half()]
        return pltpu.make_async_remote_copy(
            src_ref=block, dst_ref=block,
            send_sem=f_send.at[item], recv_sem=f_recv.at[item],
            device_id={"rep": partner}, device_id_type=MESH)

    def p_copy(c):
        return pltpu.make_async_remote_copy(
            src_ref=sbuf.at[1 - par, :, rows_of(c)], dst_ref=pbuf.at[:, rows_of(c)],
            send_sem=p_send.at[c], recv_sem=p_recv.at[c],
            device_id={"fs": mate}, device_id_type=MESH)

    def s_copy(c, k):
        return pltpu.make_async_remote_copy(
            src_ref=sbuf.at[par, z_to(k), rows_of(c)], dst_ref=rbuf.at[k, rows_of(c)],
            send_sem=s_send.at[c, k], recv_sem=s_recv.at[c, k],
            device_id={"fs": shard(z_to(k), par)}, device_id_type=MESH)

    def pair_sum(c):
        p_copy(c).wait_recv()
        for at in range(pairs):
            both = sbuf[par, at, rows_of(c)].astype(jnp.float32) + pbuf[at, rows_of(c)].astype(jnp.float32)
            sbuf[par, at, rows_of(c)] = both.astype(jnp.bfloat16)

        @pl.loop(1, pairs)
        def _(k):
            s_copy(c, k).start()

    def x_copy(c):
        return pltpu.make_async_remote_copy(
            src_ref=xs.at[rows_of(c)], dst_ref=xr.at[rows_of(c)],
            send_sem=x_send.at[c], recv_sem=x_recv.at[c],
            device_id={"rep": partner}, device_id_type=MESH)

    def c_copy(k):
        return pltpu.make_async_remote_copy(
            src_ref=cpbuf.at[me], dst_ref=cpbuf.at[me],
            send_sem=c_send.at[k], recv_sem=c_recv.at[k],
            device_id={"fs": to(k)}, device_id_type=MESH)

    def cx_copy():
        return pltpu.make_async_remote_copy(
            src_ref=cps, dst_ref=cpx, send_sem=cx_send, recv_sem=cx_recv,
            device_id={"rep": partner}, device_id_type=MESH)

    def n_copy(k):
        return pltpu.make_async_remote_copy(
            src_ref=rnbuf.at[me], dst_ref=rnbuf.at[me],
            send_sem=n_send.at[k], recv_sem=n_recv.at[k],
            device_id={"fs": to(k)}, device_id_type=MESH)

    barrier = pltpu.get_barrier_semaphore()

    @pl.loop(1, fs)
    def _(k):
        pl.semaphore_signal(barrier, inc=1, device_id={"fs": to(k)}, device_id_type=MESH)

    pl.semaphore_signal(barrier, inc=1, device_id={"rep": partner}, device_id_type=MESH)
    pl.semaphore_wait(barrier, fs)

    y_first().start()

    @pl.loop(1, pairs)
    def _(k):
        w_copy(k).start()

    wbuf[me] = w_ref[...]

    @pl.loop(0, chunks)
    def _(c):
        cols = rows_of(c)
        gate_pre = conv_chunk(
            pg_ref[:, cols].astype(jnp.float32), tg_ref[:, cols], bg_ref[:, cols])
        linear_pre = conv_chunk(
            pl_ref[:, cols].astype(jnp.float32), tl_ref[:, cols], bl_ref[:, cols])
        hidden = (gate_pre * jax.nn.sigmoid(gate_pre) * linear_pre).astype(jnp.bfloat16)
        for j in range(fs):
            part = lax.dot_general(
                hidden, og_ref[:, j * dc:(j + 1) * dc], (((0,), (0,)), ((), ())),
                preferred_element_type=jnp.float32)
            sbuf[j % 2, j // 2, cols] = part.astype(jnp.bfloat16)

        p_copy(c).start()

        @pl.when(c >= lag)
        def _():
            pair_sum(c - lag)

        for step in range(per):
            k = c * per + step + 1

            @pl.when(k < pairs)
            def _():
                w_copy(k).wait_recv()
                y_copy(k).start()
                f_copy(k).start()

            @pl.when((k >= pairs) & (k < fs))
            def _():
                y_copy(k - pairs).wait_recv()
                f_copy(k).start()

    @pl.loop(1, fs)
    def _(k):
        f_copy(k).wait_recv()

    @pl.loop(0, chunks)
    def _(c):
        cols = rows_of(c)
        gate_in = pg_ref[:, cols].astype(jnp.float32)
        linear_in = pl_ref[:, cols].astype(jnp.float32)
        taps_gate, taps_linear = tg_ref[:, cols], tl_ref[:, cols]
        gate_pre = conv_chunk(gate_in, taps_gate, bg_ref[:, cols])
        linear_pre = conv_chunk(linear_in, taps_linear, bl_ref[:, cols])
        sigma = jax.nn.sigmoid(gate_pre)
        grad_hidden = jnp.zeros((tokens, chunk), jnp.float32)
        for j in range(fs):
            grad_hidden += lax.dot_general(
                og_ref[:, j * dc:(j + 1) * dc], wbuf[j, cols], (((1,), (1,)), ((), ())),
                preferred_element_type=jnp.float32)
        grad_gate_pre = grad_hidden * linear_pre * sigma * (1.0 + gate_pre * (1.0 - sigma))
        grad_linear_pre = grad_hidden * (gate_pre * sigma)
        gg_ref[:, cols] = conv_back_chunk(grad_gate_pre, taps_gate).astype(jnp.bfloat16)
        gl_ref[:, cols] = conv_back_chunk(grad_linear_pre, taps_linear).astype(jnp.bfloat16)
        for j in range(3):
            cpbuf[me, j:j + 1, cols] = jnp.sum(
                grad_gate_pre * shift_down(gate_in, 2 - j), axis=0, keepdims=True)
            cpbuf[me, j + 3:j + 4, cols] = jnp.sum(
                grad_linear_pre * shift_down(linear_in, 2 - j), axis=0, keepdims=True)
        cpbuf[me, 6:7, cols] = jnp.sum(grad_gate_pre, axis=0, keepdims=True)
        cpbuf[me, 7:8, cols] = jnp.sum(grad_linear_pre, axis=0, keepdims=True)

        @pl.when(c == chunks - 1)
        def _():
            @pl.loop(1, fs)
            def _(k):
                c_copy(k).start()

        @pl.when(c < lag)
        def _():
            pair_sum(chunks - lag + c)

        total = sbuf[par, z, cols].astype(jnp.float32)
        for k in range(1, pairs):
            s_copy(c, k).wait_recv()
            total += rbuf[k, cols].astype(jnp.float32)
        xs[cols] = total
        x_copy(c).start()

    @pl.loop(1, fs)
    def _(k):
        c_copy(k).wait_recv()

    sums = cpbuf[0]
    for j in range(1, fs):
        sums += cpbuf[j]
    cps[...] = sums
    cx_copy().start()

    @pl.loop(0, chunks)
    def _(c):
        rows = rows_of(c)
        x_copy(c).wait_recv()
        total = xs[rows] + xr[rows]
        gd_ref[rows] = total
        square = total * total
        while square.shape[1] % 256 == 0:
            middle = square.shape[1] // 2
            square = square[:, :middle] + square[:, middle:]
        rnbuf[me, 0:1, rows] = jnp.sum(square.T, axis=0, keepdims=True)

    @pl.loop(1, fs)
    def _(k):
        n_copy(k).start()

    cx_copy().wait_recv()
    cp_ref[...] = cps[...] + cpx[...]

    @pl.loop(1, fs)
    def _(k):
        n_copy(k).wait_recv()

    norms = rnbuf[0]
    for j in range(1, fs):
        norms += rnbuf[j]
    rn_ref[...] = norms

    cx_copy().wait_send()
    y_first().wait_send()

    @pl.loop(1, pairs)
    def _(k):
        w_copy(k).wait_send()
        y_copy(k).wait_send()

    @pl.loop(1, fs)
    def _(k):
        f_copy(k).wait_send()
        c_copy(k).wait_send()
        n_copy(k).wait_send()

    @pl.loop(0, chunks)
    def _(c):
        x_copy(c).wait_send()
        p_copy(c).wait_send()

        @pl.loop(1, pairs)
        def _(k):
            s_copy(c, k).wait_send()


def out_kernel(gg, gl, cp, gd, rn, ogg, ogl, otg, otl, obg, obl, ogd, orn, sem):
    parts = sem.shape[1]
    copies = []
    for i, (source, target) in enumerate(((gg, ogg), (gl, ogl), (gd, ogd))):
        size = source.shape[0] // parts
        for j in range(parts):
            rows = pl.ds(j * size, size)
            copies.append(pltpu.make_async_copy(source.at[rows], target.at[rows], sem.at[i, j]))
    for copy in copies:
        copy.start()
    otg[...] = cp[0:3]
    otl[...] = cp[3:6]
    obg[...] = cp[6:7]
    obl[...] = cp[7:8]
    width = rn.shape[1]
    for i in range(rn.shape[0]):
        orn[0:1, i * width:(i + 1) * width] = rn[i:i + 1]
    for copy in copies:
        copy.wait()


def put_out(gg, gl, cp, gd, rn):
    ff = gg.shape[1]
    f32 = jnp.float32
    vmem = pl.BlockSpec(memory_space=pltpu.VMEM)
    hbm = pl.BlockSpec(memory_space=pl.ANY)
    row = jax.ShapeDtypeStruct((1, ff), f32)
    taps = jax.ShapeDtypeStruct((3, ff), f32)
    ogg, ogl, otg, otl, obg, obl, ogd, orn = pl.pallas_call(
        out_kernel,
        out_shape=(
            jax.ShapeDtypeStruct(gg.shape, gg.dtype), jax.ShapeDtypeStruct(gl.shape, gl.dtype),
            taps, taps, row, row, jax.ShapeDtypeStruct(gd.shape, gd.dtype), row),
        in_specs=[vmem] * 5,
        out_specs=(hbm, hbm, vmem, vmem, vmem, vmem, hbm, vmem),
        scratch_shapes=[pltpu.SemaphoreType.DMA((3, 4))],
        compiler_params=pltpu.CompilerParams(vmem_limit_bytes=2 << 20),
    )(*[pltpu.with_memory_space_constraint(value, pltpu.VMEM) for value in (gg, gl, cp, gd, rn)])
    return ogg, ogl, otg, otl, obg[0], obl[0], ogd, orn[0]


def direct_local(
    fs, pre_gate, pre_linear, taps_gate, taps_linear, bias_gate, bias_linear, down_weight, out_grad
):
    tokens, ff = pre_gate.shape
    dc = down_weight.shape[1]
    chunk = 256
    chunks = ff // chunk
    pairs = fs // 2
    f32, bf16 = jnp.float32, jnp.bfloat16
    vmem = pl.BlockSpec(memory_space=pltpu.VMEM)
    dma = pltpu.SemaphoreType.DMA
    gg, gl, cp, gd, rn = pl.pallas_call(
        functools.partial(kernel, fs, chunk),
        out_shape=(
            pltpu.VMEM((tokens, ff), bf16),
            pltpu.VMEM((tokens, ff), bf16),
            pltpu.VMEM((8, ff), f32),
            pltpu.VMEM((ff, dc), f32),
            pltpu.VMEM((1, ff), f32),
        ),
        in_specs=[vmem] * 8,
        out_specs=(vmem,) * 5,
        scratch_shapes=[
            pltpu.VMEM((fs, ff, dc), bf16),
            pltpu.VMEM((2, pairs, ff, dc), bf16),
            pltpu.VMEM((pairs, ff, dc), bf16),
            pltpu.VMEM((pairs, ff, dc), bf16),
            pltpu.VMEM((ff, dc), f32),
            pltpu.VMEM((ff, dc), f32),
            pltpu.VMEM((fs, 8, ff), f32),
            pltpu.VMEM((8, ff), f32),
            pltpu.VMEM((8, ff), f32),
            pltpu.VMEM((fs, 1, ff), f32),
            dma((pairs,)), dma((pairs,)), dma((pairs,)), dma((pairs,)),
            dma((chunks,)), dma((chunks,)), dma((fs,)), dma((fs,)),
            dma((chunks, pairs)), dma((chunks, pairs)), dma((chunks,)), dma((chunks,)),
            dma((fs,)), dma((fs,)), dma, dma, dma((fs,)), dma((fs,)),
        ],
        compiler_params=pltpu.CompilerParams(
            collective_id=0, has_side_effects=True, vmem_limit_bytes=52 << 20),
    )(pre_gate, pre_linear, taps_gate, taps_linear, bias_gate[None], bias_linear[None],
      down_weight, out_grad)
    return put_out(gg, gl, cp, gd, rn)


def line_kernel(
    fs, unit,
    pg_hbm, pl_hbm, tg_ref, tl_ref, bg_ref, bl_ref, w_hbm, og_hbm,
    gg_ref, gl_ref, cp_ref, gd_ref, rn_ref,
    og, pg, pln, wbuf, xs, xr, own, zb, ys, yr, fsum, fr, cpl, cpr, nrm, blk, tail,
    in_sem, og_sem, w_sem, x_send, x_recv, wz_send, wz_recv, wy_send, wy_recv,
    z_send, z_recv, y_send, y_recv, a_send, a_recv, f_send, f_recv,
    c_send, c_recv, b_send, b_recv, t_send, t_recv,
):
    me = lax.axis_index("fs")
    rep = lax.axis_index("rep")
    partner = 1 - rep
    nz = fs // 2
    peers = 2 * fs
    z = me // 2
    y = me % 2
    mate = me + 1 - 2 * y
    flat = rep * fs + me
    tokens, ff = pg_hbm.shape
    dc = w_hbm.shape[1]
    units = ff // unit
    half = unit // 2
    chunks = 2 * units
    split = chunks - 2
    spare = chunks + 2
    ch = half // 2
    span = ff // peers
    owners = (units - 1) * unit // span
    wch = unit // 2

    def unit_cols(u):
        return pl.ds(pl.multiple_of(u * unit, unit), unit)

    def half_cols(u, side):
        return pl.ds(pl.multiple_of(u * unit + side * half, half), half)

    def chunk_rows(c, side):
        start = (c // 2) * unit + side * half + (c % 2) * ch
        return pl.ds(pl.multiple_of(start, ch), ch)

    def w_rows(k):
        return pl.ds(pl.multiple_of(k * wch, wch), wch)

    def peer(k):
        at = lax.rem(flat + k, peers)
        return {"rep": at // fs, "fs": at % fs}

    def remote(source, target, send, recv, device):
        return pltpu.make_async_remote_copy(
            src_ref=source, dst_ref=target, send_sem=send, recv_sem=recv,
            device_id=device, device_id_type=MESH)

    def in_copies(u):
        cols = unit_cols(u)
        return (
            pltpu.make_async_copy(pg_hbm.at[:, cols], pg.at[:, cols], in_sem.at[0, u]),
            pltpu.make_async_copy(pl_hbm.at[:, cols], pln.at[:, cols], in_sem.at[1, u]))

    def og_copy():
        return pltpu.make_async_copy(og_hbm, og, og_sem)

    def w_copy():
        return pltpu.make_async_copy(w_hbm, wbuf.at[me], w_sem)

    def x_copy(c):
        return remote(xs.at[c], xr.at[c], x_send, x_recv.at[c], {"rep": partner})

    def wz_copy(way, k, src):
        block = wbuf.at[src * 2 + y, w_rows(k)]
        to = z + 1 if way == 0 else z - 1
        return remote(block, block, wz_send, wz_recv.at[k, src], {"fs": to * 2 + y})

    def wy_copy(k, src):
        block = wbuf.at[src * 2 + y, w_rows(k)]
        return remote(block, block, wy_send, wy_recv.at[k // 2], {"fs": mate})

    def z_up(c, i):
        return remote(
            zb.at[c, i], zb.at[c, i], z_send, z_recv.at[c, i], {"fs": (z + 1) * 2 + y})

    def z_down(c, i):
        slot = jnp.where(i == z - 1, nz, i)
        return remote(
            zb.at[c, i], zb.at[c, slot], z_send, z_recv.at[c, slot], {"fs": (z - 1) * 2 + y})

    def z_arrived(c, slot):
        block = zb.at[c, slot]
        remote(block, block, z_send, z_recv.at[c, slot], {"fs": mate}).wait_recv()

    def all_sent(block, send):
        remote(block, block, send, x_recv.at[0], {"fs": mate}).wait_send()

    def all_arrived(block, recv):
        remote(block, block, x_send, recv, {"fs": mate}).wait_recv()

    def y_copy(c):
        return remote(ys.at[c], yr.at[c], y_send, y_recv.at[c], {"fs": mate})

    def a_copy(c):
        rows = chunk_rows(c, rep)
        return remote(gd_ref.at[rows], gd_ref.at[rows], a_send, a_recv, {"rep": partner})

    def f_copy(f):
        return remote(fsum.at[f], fr.at[f], f_send, f_recv, {"rep": partner})

    def c_copy(k):
        at = lax.rem(flat + k, peers)
        cols = pl.ds(pl.multiple_of(at * span, span), span)
        return remote(cpl.at[:, cols], cpr.at[flat], c_send, c_recv, peer(k))

    def my_span():
        return pl.ds(pl.multiple_of(flat * span, span), span)

    def b_copy(k):
        return remote(blk.at[flat], blk.at[flat], b_send, b_recv, peer(k))

    def t_copy(k):
        return remote(tail.at[flat], tail.at[flat], t_send, t_recv, peer(k))

    barrier = pltpu.get_barrier_semaphore()

    @pl.loop(1, peers)
    def _(k):
        pl.semaphore_signal(barrier, inc=1, device_id=peer(k), device_id_type=MESH)

    w_copy().start()
    for copy in in_copies(0):
        copy.start()
    og_copy().start()

    @pl.loop(1, units)
    def _(u):
        for copy in in_copies(u):
            copy.start()

    def hidden_half(cols):
        gate_pre = conv_chunk(pg[:, cols].astype(jnp.float32), tg_ref[:, cols], bg_ref[:, cols])
        linear_pre = conv_chunk(pln[:, cols].astype(jnp.float32), tl_ref[:, cols], bl_ref[:, cols])
        return (gate_pre * jax.nn.sigmoid(gate_pre) * linear_pre).astype(jnp.bfloat16)

    def forward(u):
        for copy in in_copies(u):
            copy.wait()
        last = u == units - 1
        mine_at = jnp.where(last, split + 2 * rep, 2 * u)
        theirs_at = jnp.where(last, split + 2 * partner, spare)
        hidden = jnp.concatenate(
            [hidden_half(half_cols(u, rep)), hidden_half(half_cols(u, partner))], axis=1)
        for j in range(fs):
            part = lax.dot_general(
                hidden, og[:, j * dc:(j + 1) * dc], (((0,), (0,)), ((), ())),
                preferred_element_type=jnp.float32)
            for h in range(2):
                theirs = part[half + h * ch:half + (h + 1) * ch]
                own[mine_at + h, j // 2, j % 2] = part[h * ch:(h + 1) * ch]
                own[theirs_at + h, j // 2, j % 2] = theirs
                xs[2 * u + h, j // 2, j % 2] = theirs.astype(jnp.bfloat16)
    def backward(u):
        cols = unit_cols(u)
        all_arrived(wbuf.at[pl.ds(0, nz), cols], wy_recv.at[u])
        gate_in = pg[:, cols].astype(jnp.float32)
        linear_in = pln[:, cols].astype(jnp.float32)
        taps_gate, taps_linear = tg_ref[:, cols], tl_ref[:, cols]
        gate_pre = conv_chunk(gate_in, taps_gate, bg_ref[:, cols])
        linear_pre = conv_chunk(linear_in, taps_linear, bl_ref[:, cols])
        sigma = jax.nn.sigmoid(gate_pre)
        grad_hidden = jnp.zeros((tokens, unit), jnp.float32)
        for j in range(fs):
            grad_hidden += lax.dot_general(
                og[:, j * dc:(j + 1) * dc], wbuf[j, cols], (((1,), (1,)), ((), ())),
                preferred_element_type=jnp.float32)
        grad_gate_pre = grad_hidden * linear_pre * sigma * (1.0 + gate_pre * (1.0 - sigma))
        grad_linear_pre = grad_hidden * (gate_pre * sigma)
        gg_ref[:, cols] = conv_back_chunk(grad_gate_pre, taps_gate).astype(jnp.bfloat16)
        gl_ref[:, cols] = conv_back_chunk(grad_linear_pre, taps_linear).astype(jnp.bfloat16)
        for j in range(3):
            cpl[j:j + 1, cols] = jnp.sum(
                grad_gate_pre * shift_down(gate_in, 2 - j), axis=0, keepdims=True)
            cpl[j + 3:j + 4, cols] = jnp.sum(
                grad_linear_pre * shift_down(linear_in, 2 - j), axis=0, keepdims=True)
        cpl[6:7, cols] = jnp.sum(grad_gate_pre, axis=0, keepdims=True)
        cpl[7:8, cols] = jnp.sum(grad_linear_pre, axis=0, keepdims=True)
        count = unit // span
        for b in range(count):
            k = lax.rem(u * count + b - flat + peers, peers)

            @pl.when((k != 0) & (u < units - 1))
            def _():
                c_copy(k).start()

    def own_z(k):
        @pl.when(z < nz - 1)
        def _():
            wz_copy(0, k, z).start()

        @pl.when(z > 0)
        def _():
            wz_copy(1, k, z).start()

    def weights(t):
        @pl.when(t + ahead_z < chunks)
        def _():
            own_z(t + ahead_z)

        @pl.when(t + ahead_y < chunks)
        def _():
            wy_copy(t + ahead_y, z).start()

        for d in range(1, nz):
            k = t - d
            live = (k >= 0) & (k < chunks)

            @pl.when(live & (z >= d))
            def _():
                wz_copy(0, k, z - d).wait_recv()

                @pl.when(z < nz - 1)
                def _():
                    wz_copy(0, k, z - d).start()

                wy_copy(k, z - d).start()

            @pl.when(live & (z + d < nz))
            def _():
                wz_copy(1, k, z + d).wait_recv()

                @pl.when(z > 0)
                def _():
                    wz_copy(1, k, z + d).start()

                wy_copy(k, z + d).start()

    def add_step(c, s):
        up = z + nz - s
        down = z - nz + s

        @pl.when(z <= s - 1)
        def _():
            total = own[c, up]

            @pl.when(z > 0)
            def _():
                z_arrived(c, up)
                zb[c, up] = (total + zb[c, up].astype(jnp.float32)).astype(jnp.bfloat16)

            @pl.when(z == 0)
            def _():
                zb[c, up] = total.astype(jnp.bfloat16)

            z_up(c, up).start()

        @pl.when(z >= nz - s)
        def _():
            total = own[c, down]

            @pl.when(z < nz - 1)
            def _():
                z_arrived(c, down)
                zb[c, down] = (total + zb[c, down].astype(jnp.float32)).astype(jnp.bfloat16)

            @pl.when(z == nz - 1)
            def _():
                zb[c, down] = total.astype(jnp.bfloat16)

            z_down(c, down).start()

    def line_end(c):
        @pl.when(z > 0)
        def _():
            z_arrived(c, z)
            own[c, z] += zb[c, z].astype(jnp.float32)

        @pl.when(z < nz - 1)
        def _():
            z_arrived(c, nz)
            own[c, z] += zb[c, nz].astype(jnp.float32)

        ys[c] = own[c, z, 1 - y].astype(jnp.bfloat16)
        y_copy(c).start()

    def finish(c):
        y_copy(c).wait_recv()
        gd_ref[chunk_rows(c, rep)] = own[c, z, y] + yr[c].astype(jnp.float32)
        a_copy(c).start()

        @pl.when(c % 2 == 1)
        def _():
            norms_of(c // 2)

    def norms_of(u):
        total = gd_ref[half_cols(u, rep)]
        square = total * total
        while square.shape[1] % 256 == 0:
            middle = square.shape[1] // 2
            square = square[:, :middle] + square[:, middle:]
        nrm[pl.ds(u, 1)] = jnp.sum(square.T, axis=0, keepdims=True)

    def finish_both(f):
        c = split + f
        y_copy(c).wait_recv()
        fsum[f] = own[c, z, y] + yr[c].astype(jnp.float32)
        f_copy(f).start()

    def join_both():
        all_arrived(fr, f_recv)
        for f in range(4):
            rows = chunk_rows(split + f % 2, f // 2)
            gd_ref[rows] = fsum[f] + fr[f]
        norms_of(units - 1)

    lag = 2
    back_lag = 5
    ahead_y = 5
    ahead_z = 2
    ticks = max(split + lag + nz, chunks - 1 + back_lag)

    def send_half(u):
        x_copy(2 * u).start()
        x_copy(2 * u + 1).start()

    def reduce_params():
        cpr[flat] = cpl[:, my_span()]

        all_arrived(cpr.at[pl.ds(0, peers - 1)], c_recv)
        sums = cpr[0]
        for j in range(1, peers):
            sums += cpr[j]
        blk[flat] = sums

        @pl.loop(1, peers)
        def _(k):
            b_copy(k).start()

    w_copy().wait()
    tail[flat] = jnp.zeros(tail.shape[1:], jnp.float32)
    pl.semaphore_wait(barrier, peers - 1)
    for k in range(ahead_z):
        own_z(k)
    for k in range(ahead_y):
        wy_copy(k, z).start()
    og_copy().wait()
    forward(0)
    send_half(0)

    @pl.loop(0, ticks)
    def _(t):
        weights(t)

        slack = jnp.where(t < units + back_lag + 1, 2, jnp.where(t < 2 * units + back_lag - 4, 1, 0))
        late = t - back_lag - slack

        @pl.when((late >= 0) & (late % 2 == 0) & (late < chunks))
        def _():
            backward(late // 2)

        c = t - lag - nz

        @pl.when((c >= 0) & (c < split))
        def _():
            finish(c)

        c = t - lag - nz + 1

        @pl.when((c >= 0) & (c < split))
        def _():
            line_end(c)

        for s in range(nz - 1, 0, -1):
            c = t - lag - s + 1

            @pl.when((c >= 0) & (c < split))
            def _():
                if s == 1:
                    x_copy(c).wait_recv()
                    own[c] += xr[c].astype(jnp.float32)
                add_step(c, s)

        @pl.loop(0, 4)
        def _(f):
            s = t - 2 * f

            @pl.when(s == nz + 1)
            def _():
                finish_both(f)

            @pl.when(s == nz)
            def _():
                line_end(split + f)

            @pl.when((s >= 1) & (s < nz))
            def _():
                add_step(split + f, s)

        @pl.when(t < units - 1)
        def _():
            forward(jnp.where(t == 0, units - 1, t))

            @pl.when(t > 0)
            def _():
                send_half(t)

        @pl.when((t == ticks - 2) & (flat < owners))
        def _():
            reduce_params()

    join_both()
    tail[flat, 0:8] = cpl[:, ff - unit:]
    tail[flat, 8:, 0:half] = nrm[...]

    @pl.loop(1, peers)
    def _(k):
        t_copy(k).start()

    all_sent(xs.at[pl.ds(0, split)], x_send)
    all_sent(fsum, f_send)
    all_sent(ys, y_send)
    all_sent(zb.at[:, pl.ds(0, nz - 1)], z_send)
    all_sent(wbuf.at[pl.ds(0, nz)], wy_send)

    @pl.when((z == 0) | (z == nz - 1))
    def _():
        all_sent(wbuf.at[0], wz_send)

    @pl.when((z > 0) & (z < nz - 1))
    def _():
        all_sent(wbuf.at[pl.ds(0, nz + 1)], wz_send)

    @pl.when(flat < owners)
    def _():
        all_sent(cpr.at[pl.ds(0, owners - 1)], c_send)
        all_sent(blk.at[pl.ds(0, peers - 1)], b_send)
        all_arrived(blk.at[pl.ds(0, owners - 1)], b_recv)

    @pl.when(flat >= owners)
    def _():
        all_sent(cpr.at[pl.ds(0, owners)], c_send)
        all_arrived(blk.at[pl.ds(0, owners)], b_recv)

    for q in range(owners):
        cp_ref[:, q * span:(q + 1) * span] = blk[q]
    all_arrived(tail.at[pl.ds(0, peers - 1)], t_recv)
    sums = tail[0, 0:8]
    for q in range(1, peers):
        sums += tail[q, 0:8]
    cp_ref[:, ff - unit:] = sums
    for side in range(2):
        norms = tail[side * fs, 8:, 0:half]
        for j in range(1, fs):
            norms += tail[side * fs + j, 8:, 0:half]
        rn_ref[:, side * half:(side + 1) * half] = norms

    all_arrived(gd_ref.at[pl.ds(0, split * ch)], a_recv)
    all_sent(gd_ref.at[pl.ds(0, split * ch)], a_send)
    all_sent(tail.at[pl.ds(0, peers - 1)], t_send)


def line_local(
    fs, pre_gate, pre_linear, taps_gate, taps_linear, bias_gate, bias_linear, down_weight, out_grad
):
    tokens, ff = pre_gate.shape
    dc = down_weight.shape[1]
    unit = 256
    units = ff // unit
    chunks = 2 * units
    ch = unit // 4
    nz = fs // 2
    peers = 2 * fs
    f32, bf16 = jnp.float32, jnp.bfloat16
    vmem = pl.BlockSpec(memory_space=pltpu.VMEM)
    hbm = pl.BlockSpec(memory_space=pl.ANY)
    dma = pltpu.SemaphoreType.DMA
    gg, gl, cp, gd, rn = pl.pallas_call(
        functools.partial(line_kernel, fs, unit),
        out_shape=(
            pltpu.VMEM((tokens, ff), bf16),
            pltpu.VMEM((tokens, ff), bf16),
            pltpu.VMEM((8, ff), f32),
            pltpu.VMEM((ff, dc), f32),
            pltpu.VMEM((units, unit), f32),
        ),
        in_specs=[hbm, hbm, vmem, vmem, vmem, vmem, hbm, hbm],
        out_specs=(vmem,) * 5,
        scratch_shapes=[
            pltpu.VMEM((tokens, out_grad.shape[1]), bf16),
            pltpu.VMEM((tokens, ff), bf16),
            pltpu.VMEM((tokens, ff), bf16),
            pltpu.VMEM((fs, ff, dc), bf16),
            pltpu.VMEM((chunks, nz, 2, ch, dc), bf16),
            pltpu.VMEM((chunks - 2, nz, 2, ch, dc), bf16),
            pltpu.VMEM((chunks + 4, nz, 2, ch, dc), f32),
            pltpu.VMEM((chunks + 2, nz + 1, 2, ch, dc), bf16),
            pltpu.VMEM((chunks + 2, ch, dc), bf16),
            pltpu.VMEM((chunks + 2, ch, dc), bf16),
            pltpu.VMEM((4, ch, dc), f32),
            pltpu.VMEM((4, ch, dc), f32),
            pltpu.VMEM((8, ff), f32),
            pltpu.VMEM((peers, 8, ff // peers), f32),
            pltpu.VMEM((units, unit // 2), f32),
            pltpu.VMEM((peers, 8, ff // peers), f32),
            pltpu.VMEM((peers, 8 + units, unit), f32),
            dma((2, units)), dma, dma,
            dma, dma((chunks,)), dma, dma((chunks, nz)), dma, dma((units,)),
            dma, dma((chunks + 2, nz + 1)), dma, dma((chunks + 2,)), dma, dma, dma, dma,
            dma, dma, dma, dma, dma, dma,
        ],
        compiler_params=pltpu.CompilerParams(
            collective_id=0, has_side_effects=True, vmem_limit_bytes=55 << 20),
    )(pre_gate, pre_linear, taps_gate, taps_linear, bias_gate[None], bias_linear[None],
      down_weight, out_grad)
    return put_out(gg, gl, cp, gd, rn)


def on_a_line(fs, ff, dc):
    nz = fs // 2
    return (
        fs % 2 == 0 and 2 <= nz <= 4 and ff % (256 * fs) == 0
        and 1536 <= ff <= 512 * fs and dc % 128 == 0)


def local(fs, *args):
    if on_a_line(fs, args[0].shape[1], args[6].shape[1]):
        return line_local(fs, *args)
    return direct_local(fs, *args)


def solution(mesh):
    in_specs = (
        P(("rep", "fs"), "tp"),
        P(("rep", "fs"), "tp"),
        P(None, "tp"),
        P(None, "tp"),
        P("tp"),
        P("tp"),
        P("tp", "fs"),
        P(("rep", "fs"), None),
    )
    out_specs = (
        P(("rep", "fs"), "tp"),
        P(("rep", "fs"), "tp"),
        P(None, "tp"),
        P(None, "tp"),
        P("tp"),
        P("tp"),
        P("tp", "fs"),
        P("tp"),
    )
    return jax.shard_map(
        functools.partial(local, mesh.shape["fs"]), mesh=mesh, in_specs=in_specs, out_specs=out_specs, check_vma=False)
```
